256 devices in a mesh: ra: 32 (over z, y), cb: 4 (over x), dp: 2 (over core).
Axes of the slice: x: 4, y: 4, z: 8, core: 2. Of those that a mesh axis runs over, the one named last changes fastest.
Arguments:
- stream: bfloat16 [3072, 4096], P(('cb', 'dp'), 'ra'), may hold values from -20 to 20
- up_first: bfloat16 [4096, 16384], P('cb', 'ra'), may hold values from -0.09375 to 0.09375
- down_first: bfloat16 [16384, 4096], P('ra', 'cb'), may hold values from -0.046875 to 0.046875
- up_second: bfloat16 [4096, 16384], P('cb', 'ra'), may hold values from -0.09375 to 0.09375
- down_second: bfloat16 [16384, 4096], P('ra', 'cb'), may hold values from -0.046875 to 0.046875
- gain_first: float32 [4096], P('ra'), may hold values from 0.1 to 1.9
- bias_first: float32 [4096], P('ra'), may hold values from -3 to 3
- gain_second: float32 [4096], P('ra'), may hold values from 0.1 to 1.9
- bias_second: float32 [4096], P('ra'), may hold values from -3 to 3
Outputs:
- result: bfloat16 [3072, 4096], P(('cb', 'dp'), 'ra')
The draws below stay inside these ranges and needn't reach their ends.
All inputs are finite; a program needn't handle non-finite values.
Results may differ from the reference program's by a relative error of at most 0.0093.
Values may be sent and summed in bfloat16 or wider, within the bound.
No kernel may reach another device: no remote copies, remote signals or barrier semaphores. Data moves between devices by JAX's collectives and lax.ppermute only.
A program may use at most 64 MiB of HBM per device.

```python
import jax
import jax.numpy as jnp
from jax import lax

D = 4096
FF = 16384
TOKENS = 3072


def draw_stream(key, part):
    k_perm, k_base, k_rows = jax.random.split(key, 3)
    levels = jnp.array([0.35, 0.7, 1.4, 2.8], jnp.float32)[jax.random.permutation(k_perm, 4)]
    band = jnp.arange(D) * 4 // D
    column_scale = levels[band]
    base = jax.random.normal(k_base, (TOKENS, D), jnp.float32)
    offset = 0.5 * jax.random.normal(k_rows, (TOKENS, 1), jnp.float32)
    values = jnp.clip(base * column_scale[None, :] + offset, -20.0, 20.0)
    return values.astype(jnp.bfloat16)


def block_scale(own_key, shape, shards, least, high):
    level, own = 1.0, jax.random.fold_in(own_key, 6)
    for axis_at, shards_of in shards:
        steps = jnp.exp(jax.random.uniform(jax.random.fold_in(own, axis_at), (shards_of,), jnp.float32, least / len(shards), high / len(shards)))
        level = level * jnp.repeat(steps, shape[axis_at] // shards_of).reshape([-1 if axis == axis_at else 1 for axis in range(len(shape))])
    return level


def bell_draw(rng, shape, scale, reach, pieces=(), held_as=jnp.bfloat16):
    level = block_scale(rng, shape, pieces, -0.22, 0.18) if pieces else 1.0
    drawn = jax.random.normal(rng, shape, jnp.float32) * scale * level
    return jnp.minimum(jnp.maximum(drawn, -reach), reach).astype(held_as)


def setup_inputs(seed: int = 0) -> dict:
    key_of = jax.random.split(jax.random.key(seed), 10)
    stream = draw_stream(jax.random.fold_in(key_of[9], 71), 0)
    up_first = bell_draw(key_of[1], (D, FF), D ** -0.5, 0.09375, ((0, 4), (1, 32)))
    down_first = bell_draw(key_of[2], (FF, D), FF ** -0.5, 0.046875, ((0, 32), (1, 4)))
    up_second = bell_draw(key_of[3], (D, FF), D ** -0.5, 0.09375, ((0, 4), (1, 32)))
    down_second = bell_draw(key_of[4], (FF, D), FF ** -0.5, 0.046875, ((0, 32), (1, 4)))
    gain_first = jnp.clip(1.0 + 0.18 * jax.random.normal(key_of[5], (D,), jnp.float32), 0.1, 1.9)
    bias_first = bell_draw(key_of[6], (D,), 0.5, 3.0, ((0, 32),), jnp.float32)
    gain_second = jnp.clip(1.0 + 0.18 * jax.random.normal(key_of[7], (D,), jnp.float32), 0.1, 1.9)
    bias_second = bell_draw(key_of[8], (D,), 0.5, 3.0, ((0, 32),), jnp.float32)
    return dict(stream=stream, up_first=up_first, down_first=down_first, up_second=up_second, down_second=down_second, gain_first=gain_first, bias_first=bias_first, gain_second=gain_second, bias_second=bias_second)


RESID = 1.4142135
EPS = 0.5

def normalize(mixed, gain, bias):
    mean = lax.optimization_barrier(jnp.mean(mixed, axis=1, keepdims=True))
    centered = mixed - mean
    var = lax.optimization_barrier(jnp.mean(centered * centered, axis=1, keepdims=True))
    return centered * lax.rsqrt(var + EPS) * gain + bias

def reference(stream, up_first, down_first, up_second, down_second, gain_first, bias_first, gain_second, bias_second):
    x = stream
    for up, down, gain, bias in ((up_first, down_first, gain_first, bias_first), (up_second, down_second, gain_second, bias_second)):
        pre = jnp.dot(x, up, preferred_element_type=jnp.float32)
        hidden = jnp.square(jax.nn.relu(pre)).astype(jnp.bfloat16)
        branch = jnp.dot(hidden, down, preferred_element_type=jnp.float32)
        mixed = RESID * x.astype(jnp.float32) + branch
        x = normalize(mixed, gain, bias).astype(jnp.bfloat16)
    return x
```

```python
import functools

import jax
import jax.numpy as jnp
from jax import lax
from jax.experimental import pallas as pl
from jax.experimental.pallas import tpu as pltpu
from jax.sharding import Mesh
from jax.sharding import PartitionSpec as P

Z, Y, X, C = "ra_0", "ra_1", "cb", "dp"
RA = (Z, Y)
RESID = 1.4142135
EPS = 0.5
BF = jnp.bfloat16
F32 = jnp.float32


def swap(blocks, axis):
    return lax.all_to_all(blocks, axis, 0, 0, tiled=True)


def to_all(block, axis):
    return swap(jnp.broadcast_to(block[None], (lax.axis_size(axis), *block.shape)), axis)


def gathered(block):
    return to_all(to_all(block, Z), Y)


def scattered_sum(parts):
    near = jnp.sum(swap(parts, Y).astype(F32), axis=0).astype(BF)
    return jnp.sum(swap(near, Z).astype(F32), axis=0)


def shift(a, axis, by):
    n = lax.axis_size(axis)
    return lax.ppermute(a, axis, [(i, (i + by) % n) for i in range(n)])


def half_of(w):
    rows = w.shape[0] // 2
    return lax.dynamic_slice_in_dim(w, lax.axis_index(C) * rows, rows, 0)


def split3(v):
    hi = lax.reduce_precision(v, 8, 7)
    mid = lax.reduce_precision(v - hi, 8, 7)
    return [hi, mid, v - hi - mid]


def join3(rows):
    return rows[0] + rows[1] + rows[2]


def matmuls(xs, upv, dv, ov, out, out_sems, wait_up, wait_down, nx):
    wait_up()
    pre = jnp.dot(xs[...], upv[...], preferred_element_type=F32)
    hidden = jnp.square(jnp.maximum(pre, 0.0)).astype(BF)
    half = hidden.shape[1] // 2
    copies = []
    for j in range(nx):
        wait_down(j)
        part = jnp.dot(hidden[:, :half], dv[2 * j], preferred_element_type=F32)
        part = part + jnp.dot(hidden[:, half:], dv[2 * j + 1], preferred_element_type=F32)
        part = part.astype(BF)
        ny, nz = ov.shape[0], ov.shape[1] // nx
        for z in range(nz):
            for y in range(ny):
                at = (z * ny + y) * 128
                ov[y, j * nz + z] = part[:, at : at + 128]
        zs = pl.ds(j * nz, nz)
        copy = pltpu.make_async_copy(ov.at[:, zs], out.at[:, zs], out_sems.at[j])
        copy.start()
        copies.append(copy)
    for copy in copies:
        copy.wait()


def first_kernel(idx, x, up, own, m1, m2, m3, o1, o2, o3, out, xs, upv, dv, ov, x_sem, up_sem, d_sems, out_sems):
    nx = dv.shape[0] // 2
    rows = dv.shape[1]
    me, core = idx[0], idx[1]
    up_copy = pltpu.make_async_copy(up, upv, up_sem)
    tokens = xs.shape[0]
    ny, nz = x.shape[0], x.shape[1]
    x_copies = []
    for z in range(nz):
        for y in range(ny):
            at = (z * ny + y) * 128
            copy = pltpu.make_async_copy(
                x.at[y, z, pl.ds(0, tokens)], xs.at[:, pl.ds(at, 128)], x_sem.at[z * ny + y]
            )
            copy.start()
            x_copies.append(copy)
    up_copy.start()
    d_copies = [
        pltpu.make_async_copy(own.at[pl.ds(0, rows)], dv.at[2 * me], d_sems.at[0]),
        pltpu.make_async_copy(own.at[pl.ds(rows, rows)], dv.at[2 * me + 1], d_sems.at[1]),
    ]
    for i, (by, mine, other) in enumerate(((1, m1, o1), (nx - 1, m2, o2), (2, m3, o3))):
        source = lax.rem(me + (nx - by), nx)
        d_copies.append(pltpu.make_async_copy(mine, dv.at[2 * source + core], d_sems.at[2 + 2 * i]))
        d_copies.append(pltpu.make_async_copy(other, dv.at[2 * source + 1 - core], d_sems.at[3 + 2 * i]))
    for copy in d_copies:
        copy.start()

    def wait_up():
        for copy in x_copies:
            copy.wait()
        up_copy.wait()

    def wait_down(j):
        if j == 0:
            for copy in d_copies:
                copy.wait()

    matmuls(xs, upv, dv, ov, out, out_sems, wait_up, wait_down, nx)


def second_kernel(
    x, up, down, gain, bias, mixed, own_gain, own_bias, out, own, xs, xv, upv, dv, ov, x_sem, up_sem, d_sem, out_sems
):
    nx = dv.shape[0] // 2
    ny, nz = x.shape[0], x.shape[1]
    tokens = xs.shape[0]
    x_copy = pltpu.make_async_copy(x, xv, x_sem)
    up_copy = pltpu.make_async_copy(up, upv, up_sem)
    d_copy = pltpu.make_async_copy(down, dv, d_sem)
    x_copy.start()
    up_copy.start()
    d_copy.start()
    x_copy.wait()
    step = 64
    width = ny * nz * 128

    def norm(i, carry):
        rows = pl.ds(pl.multiple_of(i * step, step), step)
        acc = jnp.zeros((step, 128), F32)
        for z in range(nz):
            for y in range(ny):
                acc = acc + xv[y, z, rows, :].astype(F32)
        mean = jnp.sum(acc, axis=1, keepdims=True) / width
        acc = jnp.zeros((step, 128), F32)
        for z in range(nz):
            for y in range(ny):
                d = xv[y, z, rows, :].astype(F32) - mean
                acc = acc + d * d
        scale = lax.rsqrt(jnp.sum(acc, axis=1, keepdims=True) / width + EPS)
        for z in range(nz):
            for y in range(ny):
                b = z * ny + y
                d = (xv[y, z, rows, :].astype(F32) - mean) * scale
                xs[rows, b * 128 : (b + 1) * 128] = (d * gain[b : b + 1] + bias[b : b + 1]).astype(BF)
        own[rows, :] = ((mixed[rows, :] - mean) * scale * own_gain[...] + own_bias[...]).astype(BF)
        return carry

    lax.fori_loop(0, tokens // step, norm, 0)

    def wait_down(j):
        if j == 0:
            d_copy.wait()

    matmuls(xs, upv, dv, ov, out, out_sems, up_copy.wait, wait_down, nx)


ANY = pl.BlockSpec(memory_space=pltpu.MemorySpace.HBM)
VMEM = pl.BlockSpec(memory_space=pltpu.MemorySpace.VMEM)
SMEM = pl.BlockSpec(memory_space=pltpu.MemorySpace.SMEM)


def sizes(up, ny, nz, tokens):
    width, ff = up.shape
    out = jax.ShapeDtypeStruct((ny, nz, tokens, 128), BF)
    return width, ff, out


def first_ffn(idx, x, tokens, up, own, mine, others):
    ny, nz = x.shape[:2]
    width, ff, out = sizes(up, ny, nz, tokens)
    nx = lax.axis_size(X)
    return pl.pallas_call(
        first_kernel,
        out_shape=out,
        in_specs=[SMEM] + [ANY] * 9,
        out_specs=ANY,
        scratch_shapes=[
            pltpu.VMEM((tokens, width), BF),
            pltpu.VMEM((width, ff), BF),
            pltpu.VMEM((2 * nx, ff // 2, width // nx), BF),
            pltpu.VMEM(out.shape, BF),
            pltpu.SemaphoreType.DMA((ny * nz,)),
            pltpu.SemaphoreType.DMA,
            pltpu.SemaphoreType.DMA((8,)),
            pltpu.SemaphoreType.DMA((nx,)),
        ],
        cost_estimate=pl.CostEstimate(flops=4 * tokens * width * ff, bytes_accessed=14 << 20, transcendentals=0),
        name="first_ffn",
    )(idx, x, up, own, *mine, *others)


def second_ffn(x, up, down, gain, bias, mixed, own_gain, own_bias):
    ny, nz, tokens = x.shape[:3]
    width, ff, out = sizes(up, ny, nz, tokens)
    nx = lax.axis_size(X)
    return pl.pallas_call(
        second_kernel,
        out_shape=(out, jax.ShapeDtypeStruct((tokens, 128), BF)),
        in_specs=[ANY] * 3 + [VMEM] * 5,
        out_specs=(ANY, VMEM),
        scratch_shapes=[
            pltpu.VMEM((tokens, width), BF),
            pltpu.VMEM(x.shape, BF),
            pltpu.VMEM((width, ff), BF),
            pltpu.VMEM((2 * nx, ff // 2, width // nx), BF),
            pltpu.VMEM(out.shape, BF),
            pltpu.SemaphoreType.DMA,
            pltpu.SemaphoreType.DMA,
            pltpu.SemaphoreType.DMA,
            pltpu.SemaphoreType.DMA((nx,)),
        ],
        cost_estimate=pl.CostEstimate(flops=4 * tokens * width * ff, bytes_accessed=14 << 20, transcendentals=0),
        name="second_ffn",
    )(x, up, down, gain, bias, mixed, own_gain, own_bias)


def body(
    stream,
    up_first,
    down_first,
    up_second,
    down_second,
    gain_first,
    bias_first,
    gain_second,
    bias_second,
):
    tokens = stream.shape[0]
    half = half_of(down_first)
    mine = [shift(half, X, by) for by in (1, -1, 2)]
    up_1 = lax.all_gather(half_of(up_first), (X, C), axis=0, tiled=True)
    tail = jnp.stack(split3(gain_first) + split3(bias_first) + [jnp.zeros_like(gain_first)] * 2)
    x_all = gathered(jnp.concatenate([stream, tail.astype(BF)], axis=0))
    others = [shift(m, C, 1) for m in mine]
    up_2 = lax.all_gather(half_of(up_second), (X, C), axis=0, tiled=True)
    down_2 = lax.all_gather(half_of(down_second), (X, C), axis=0, tiled=False)
    down_2 = down_2.reshape(-1, *half.shape)
    idx = jnp.stack([lax.axis_index(X), lax.axis_index(C)]).astype(jnp.int32)
    parts = first_ffn(idx, x_all, tokens, up_1, down_first, mine, others)
    mixed = RESID * stream.astype(F32) + scattered_sum(parts)

    ny, nz = x_all.shape[:2]
    vectors = jnp.transpose(x_all[:, :, tokens:].astype(F32), (2, 1, 0, 3)).reshape(8, nz * ny, 128)
    gain, bias = join3(vectors[0:3]), join3(vectors[3:6])
    mixed_all = gathered(mixed.astype(BF))
    parts, x = second_ffn(
        mixed_all, up_2, down_2, gain, bias, mixed, gain_first[None], bias_first[None]
    )
    mixed = RESID * x.astype(F32) + scattered_sum(parts)
    width = mixed.shape[1] * lax.axis_size(RA)
    sums = jnp.concatenate([jnp.sum(mixed, axis=1), jnp.sum(mixed * mixed, axis=1)])
    sums = jnp.sum(to_all(sums[None], RA), axis=0)[0]
    mean = sums[:tokens, None] / width
    var = sums[tokens:, None] / width - mean * mean
    return ((mixed - mean) * lax.rsqrt(var + EPS) * gain_second + bias_second).astype(BF)


def solution(mesh):
    torus = Mesh(mesh.devices.reshape(8, 4, mesh.shape["cb"], mesh.shape["dp"]), (Z, Y, X, C))
    in_specs = (
        P((X, C), RA),
        P(X, RA),
        P(RA, X),
        P(X, RA),
        P(RA, X),
        P(RA),
        P(RA),
        P(RA),
        P(RA),
    )
    out_specs = P((X, C), RA)
    return jax.shard_map(body, mesh=torus, in_specs=in_specs, out_specs=out_specs, check_vma=False)
```

```python
import jax
import jax.numpy as jnp
from jax import lax
from jax.experimental import pallas as pl
from jax.experimental.pallas import tpu as pltpu
from jax.sharding import Mesh
from jax.sharding import PartitionSpec as P


Z, Y, X, C = "ra_0", "ra_1", "cb", "dp"
RA = (Z, Y)
ALL = (Z, Y, X, C)
RESID = 1.4142135
EPS = 0.5
BF = jnp.bfloat16
F32 = jnp.float32
NZ, NY = 8, 4


def place(z, y, core, nz, ny):
    z, y = (z - core) % nz, (y - core) % ny
    return (y % 2) * 2 + z % 2, (y // 2) * (nz // 2) + z // 2


def groups_of(sizes):
    nz, ny, nx, nc = sizes
    near, far = {}, {}
    for z in range(nz):
        for y in range(ny):
            for x in range(nx):
                for c in range(nc):
                    at = ((z * ny + y) * nx + x) * nc + c
                    a, b = place(z, y, c, nz, ny)
                    near.setdefault((x, c, b), {})[a] = at
                    far.setdefault((x, c, a), {})[b] = at
    return [[[m[i] for i in sorted(m)] for m in g.values()] for g in (near, far)]


def swap(blocks, groups):
    return lax.all_to_all(blocks, ALL, 0, 0, axis_index_groups=groups, tiled=True)


def to_all(block, groups):
    return swap(jnp.broadcast_to(block[None], (len(groups[0]), *block.shape)), groups)


def gathered(block, near, far):
    return to_all(to_all(block, far), near)


def scattered_sum(parts, near, far):
    some = jnp.sum(swap(parts, near).astype(F32), axis=0).astype(BF)
    return jnp.sum(swap(some, far).astype(F32), axis=0)


def stats_to_all(row):
    n = lax.axis_size(RA)
    return lax.all_to_all(jnp.broadcast_to(row[None], (n, *row.shape)), RA, 0, 0, tiled=True)


def shift(a, axis, by):
    n = lax.axis_size(axis)
    return lax.ppermute(a, axis, [(i, (i + by) % n) for i in range(n)])


def half_of(w):
    rows = w.shape[0] // 2
    return lax.dynamic_slice_in_dim(w, lax.axis_index(C) * rows, rows, 0)


def split3(v):
    hi = lax.reduce_precision(v, 8, 7)
    mid = lax.reduce_precision(v - hi, 8, 7)
    return [hi, mid, v - hi - mid]


def at_core(z, y, core, nz, ny):
    a0, b0 = place(z, y, 0, nz, ny)
    a1, b1 = place(z, y, 1, nz, ny)
    return a0 + core * (a1 - a0), b0 + core * (b1 - b0)


def matmuls(core, xs, upv, dv, ov, out, out_sems, wait_up, wait_down, nx):
    ny, nz = NY, NZ
    wait_up()
    pre = jnp.dot(xs[...], upv[...], preferred_element_type=F32)
    hidden = jnp.square(jnp.maximum(pre, 0.0)).astype(BF)
    half = hidden.shape[1] // 2
    copies = []
    for j in range(nx):
        wait_down(j)
        part = jnp.dot(hidden[:, :half], dv[2 * j], preferred_element_type=F32)
        part = part + jnp.dot(hidden[:, half:], dv[2 * j + 1], preferred_element_type=F32)
        part = part.astype(BF)
        per = nz // nx
        for zz in range(per):
            for y in range(ny):
                at = (zz * ny + y) * 128
                z = j * per + zz
                b = z * ny + y
                ov[b] = part[:, at : at + 128]
                copy = pltpu.make_async_copy(ov.at[b], out.at[at_core(z, y, core, nz, ny)], out_sems.at[b])
                copy.start()
                copies.append(copy)
    for copy in copies:
        copy.wait()


def first_kernel(
    idx, x, up, own, m1, m2, m3, o1, o2, o3, out, gain, bias, xs, tv, upv, dv, ov, x_sem, t_sem, up_sem, d_sems, out_sems
):
    nx = dv.shape[0] // 2
    rows = dv.shape[1]
    me, core = idx[0], idx[1]
    up_copy = pltpu.make_async_copy(up, upv, up_sem)
    tokens = xs.shape[0]
    ny, nz = NY, NZ
    x_copies, t_copies = [], []
    for z in range(nz):
        for y in range(ny):
            b = z * ny + y
            p, q = at_core(z, y, core, nz, ny)
            copy = pltpu.make_async_copy(
                x.at[p, q, pl.ds(0, tokens)], xs.at[:, pl.ds(b * 128, 128)], x_sem.at[b]
            )
            copy.start()
            x_copies.append(copy)
            copy = pltpu.make_async_copy(x.at[p, q, pl.ds(tokens, 8)], tv.at[b], t_sem.at[b])
            copy.start()
            t_copies.append(copy)
    up_copy.start()
    d_copies = [
        pltpu.make_async_copy(own.at[pl.ds(0, rows)], dv.at[2 * me], d_sems.at[0]),
        pltpu.make_async_copy(own.at[pl.ds(rows, rows)], dv.at[2 * me + 1], d_sems.at[1]),
    ]
    for i, (by, mine, other) in enumerate(((1, m1, o1), (nx - 1, m2, o2), (2, m3, o3))):
        source = lax.rem(me + (nx - by), nx)
        d_copies.append(pltpu.make_async_copy(mine, dv.at[2 * source + core], d_sems.at[2 + 2 * i]))
        d_copies.append(pltpu.make_async_copy(other, dv.at[2 * source + 1 - core], d_sems.at[3 + 2 * i]))
    for copy in d_copies:
        copy.start()

    def wait_up():
        for copy in x_copies:
            copy.wait()
        up_copy.wait()

    def wait_down(j):
        if j == 0:
            for copy in d_copies:
                copy.wait()

    matmuls(core, xs, upv, dv, ov, out, out_sems, wait_up, wait_down, nx)
    for b in range(nz * ny):
        t_copies[b].wait()
        t = tv[b].astype(F32)
        gain[b : b + 1] = t[0:1] + t[1:2] + t[2:3]
        bias[b : b + 1] = t[3:4] + t[4:5] + t[5:6]


def second_kernel(
    idx, x, up, down, gain, bias, mixed, own_gain, own_bias, out, own, xs, xv, upv, dv, ov, x_sem, up_sem, d_sem, out_sems
):
    nx = dv.shape[0] // 2
    ny, nz = NY, NZ
    core = idx[1]
    tokens = xs.shape[0]
    x_copies = []
    for z in range(nz):
        for y in range(ny):
            b = z * ny + y
            copy = pltpu.make_async_copy(x.at[at_core(z, y, core, nz, ny)], xv.at[b], x_sem.at[b])
            copy.start()
            x_copies.append(copy)
    up_copy = pltpu.make_async_copy(up, upv, up_sem)
    d_copy = pltpu.make_async_copy(down, dv, d_sem)
    up_copy.start()
    d_copy.start()
    for copy in x_copies:
        copy.wait()
    step = 64
    width = ny * nz * 128

    def norm(i, carry):
        rows = pl.ds(pl.multiple_of(i * step, step), step)
        acc = jnp.zeros((step, 128), F32)
        for b in range(nz * ny):
            acc = acc + xv[b, rows, :].astype(F32)
        mean = jnp.sum(acc, axis=1, keepdims=True) / width
        acc = jnp.zeros((step, 128), F32)
        for b in range(nz * ny):
            d = xv[b, rows, :].astype(F32) - mean
            acc = acc + d * d
        scale = lax.rsqrt(jnp.sum(acc, axis=1, keepdims=True) / width + EPS)
        for b in range(nz * ny):
            d = (xv[b, rows, :].astype(F32) - mean) * scale
            xs[rows, b * 128 : (b + 1) * 128] = (d * gain[b : b + 1] + bias[b : b + 1]).astype(BF)
        own[rows, :] = ((mixed[rows, :] - mean) * scale * own_gain[...] + own_bias[...]).astype(BF)
        return carry

    lax.fori_loop(0, tokens // step, norm, 0)

    def wait_down(j):
        if j == 0:
            d_copy.wait()

    matmuls(core, xs, upv, dv, ov, out, out_sems, up_copy.wait, wait_down, nx)


ANY = pl.BlockSpec(memory_space=pltpu.MemorySpace.HBM)
VMEM = pl.BlockSpec(memory_space=pltpu.MemorySpace.VMEM)
SMEM = pl.BlockSpec(memory_space=pltpu.MemorySpace.SMEM)


def first_ffn(idx, x, tokens, up, own, mine, others):
    width, ff = up.shape
    nx, nb = lax.axis_size(X), NZ * NY
    vector = jax.ShapeDtypeStruct((nb, 128), F32)
    return pl.pallas_call(
        first_kernel,
        out_shape=(jax.ShapeDtypeStruct((4, nb // 4, tokens, 128), BF), vector, vector),
        in_specs=[SMEM] + [ANY] * 9,
        out_specs=(ANY, VMEM, VMEM),
        scratch_shapes=[
            pltpu.VMEM((tokens, width), BF),
            pltpu.VMEM((nb, 8, 128), BF),
            pltpu.VMEM((width, ff), BF),
            pltpu.VMEM((2 * nx, ff // 2, width // nx), BF),
            pltpu.VMEM((nb, tokens, 128), BF),
            pltpu.SemaphoreType.DMA((nb,)),
            pltpu.SemaphoreType.DMA((nb,)),
            pltpu.SemaphoreType.DMA,
            pltpu.SemaphoreType.DMA((8,)),
            pltpu.SemaphoreType.DMA((nb,)),
        ],
        cost_estimate=pl.CostEstimate(flops=4 * tokens * width * ff, bytes_accessed=14 << 20, transcendentals=0),
        name="first_ffn",
    )(idx, x, up, own, *mine, *others)


def second_ffn(idx, x, up, down, gain, bias, mixed, own_gain, own_bias):
    tokens = x.shape[2]
    width, ff = up.shape
    nx, nb = lax.axis_size(X), NZ * NY
    return pl.pallas_call(
        second_kernel,
        out_shape=(jax.ShapeDtypeStruct(x.shape, BF), jax.ShapeDtypeStruct((tokens, 128), BF)),
        in_specs=[SMEM] + [ANY] * 3 + [VMEM] * 5,
        out_specs=(ANY, VMEM),
        scratch_shapes=[
            pltpu.VMEM((tokens, width), BF),
            pltpu.VMEM((nb, tokens, 128), BF),
            pltpu.VMEM((width, ff), BF),
            pltpu.VMEM((2 * nx, ff // 2, width // nx), BF),
            pltpu.VMEM((nb, tokens, 128), BF),
            pltpu.SemaphoreType.DMA((nb,)),
            pltpu.SemaphoreType.DMA,
            pltpu.SemaphoreType.DMA,
            pltpu.SemaphoreType.DMA((nb,)),
        ],
        cost_estimate=pl.CostEstimate(flops=4 * tokens * width * ff, bytes_accessed=14 << 20, transcendentals=0),
        name="second_ffn",
    )(idx, x, up, down, gain, bias, mixed, own_gain, own_bias)


def body(
    stream,
    up_first,
    down_first,
    up_second,
    down_second,
    gain_first,
    bias_first,
    gain_second,
    bias_second,
):
    tokens = stream.shape[0]
    near, far = groups_of([lax.axis_size(axis) for axis in ALL])
    half = half_of(down_first)
    mine = [shift(half, X, by) for by in (1, -1, 2)]
    up_1 = lax.all_gather(half_of(up_first), (X, C), axis=0, tiled=True)
    tail = jnp.stack(split3(gain_first) + split3(bias_first) + [jnp.zeros_like(gain_first)] * 2)
    x_far = to_all(jnp.concatenate([stream, tail.astype(BF)], axis=0), far)
    x_all = to_all(x_far, near)
    others = [shift(m, C, 1) for m in mine]
    up_2 = lax.all_gather(half_of(up_second), (X, C), axis=0, tiled=True)
    down_2 = lax.all_gather(half_of(down_second), (X, C), axis=0, tiled=False)
    down_2 = down_2.reshape(-1, *half.shape)
    idx = jnp.stack([lax.axis_index(X), lax.axis_index(C)]).astype(jnp.int32)
    parts, gain, bias = first_ffn(idx, x_all, tokens, up_1, down_first, mine, others)
    mixed = RESID * stream.astype(F32) + scattered_sum(parts, near, far)
    mixed_all = gathered(mixed.astype(BF), near, far)
    parts, x = second_ffn(
        idx, mixed_all, up_2, down_2, gain, bias, mixed, gain_first[None], bias_first[None]
    )
    mixed = RESID * x.astype(F32) + scattered_sum(parts, near, far)
    width = mixed.shape[1] * lax.axis_size(RA)
    sums = jnp.concatenate([jnp.sum(mixed, axis=1), jnp.sum(mixed * mixed, axis=1)])
    sums = jnp.sum(stats_to_all(sums[None]), axis=0)[0]
    mean = sums[:tokens, None] / width
    var = sums[tokens:, None] / width - mean * mean
    return ((mixed - mean) * lax.rsqrt(var + EPS) * gain_second + bias_second).astype(BF)


def solution(mesh):
    torus = Mesh(mesh.devices.reshape(NZ, NY, mesh.shape["cb"], mesh.shape["dp"]), (Z, Y, X, C))
    in_specs = (
        P((X, C), RA),
        P(X, RA),
        P(RA, X),
        P(X, RA),
        P(RA, X),
        P(RA),
        P(RA),
        P(RA),
        P(RA),
    )
    out_specs = P((X, C), RA)

    return jax.shard_map(body, mesh=torus, in_specs=in_specs, out_specs=out_specs, check_vma=False)
```

```python
import jax
import jax.numpy as jnp
from jax import lax
from jax.experimental import pallas as pl
from jax.experimental.pallas import tpu as pltpu
from jax.sharding import Mesh
from jax.sharding import PartitionSpec as P


Z, Y, X, C = "ra_0", "ra_1", "cb", "dp"
RA = (Z, Y)
ALL = (Z, Y, X, C)
RESID = 1.4142135
EPS = 0.5
BF = jnp.bfloat16
F32 = jnp.float32
NZ, NY = 8, 4


def place(z, y, core, nz, ny):
    z, y = (z - core) % nz, (y - core) % ny
    return (y % 2) * 2 + z % 2, (y // 2) * (nz // 2) + z // 2


def groups_of(sizes):
    nz, ny, nx, nc = sizes
    near, far = {}, {}
    for z in range(nz):
        for y in range(ny):
            for x in range(nx):
                for c in range(nc):
                    at = ((z * ny + y) * nx + x) * nc + c
                    a, b = place(z, y, c, nz, ny)
                    near.setdefault((x, c, b), {})[a] = at
                    far.setdefault((x, c, a), {})[b] = at
    pairs = [[(g[a], g[a ^ d]) for g in near.values() for a in range(4)] for d in range(4)]
    return pairs, [[m[i] for i in sorted(m)] for m in far.values()]


def far_swap(blocks, far):
    return lax.all_to_all(blocks, ALL, 0, 0, axis_index_groups=far, tiled=True)


def far_to_all(block, far):
    return far_swap(jnp.broadcast_to(block[None], (len(far[0]), *block.shape)), far)


def near_send(blocks, near):
    return [blocks[0]] + [lax.ppermute(blocks[d], ALL, near[d]) for d in (3, 1, 2)]


def near_swap(blocks, near):
    own, diagonal, one, two = near_send(blocks, near)
    return [own, one, two, diagonal]


def gathered(block, near, far):
    return near_swap([far_to_all(block, far)] * 4, near)


def scattered_sum(parts, near, far):
    some = sum(p.astype(F32) for p in near_swap(parts, near)).astype(BF)
    return jnp.sum(far_swap(some, far).astype(F32), axis=0)


def stats_to_all(row):
    n = lax.axis_size(RA)
    return lax.all_to_all(jnp.broadcast_to(row[None], (n, *row.shape)), RA, 0, 0, tiled=True)


def shift(a, axis, by):
    n = lax.axis_size(axis)
    return lax.ppermute(a, axis, [(i, (i + by) % n) for i in range(n)])


def half_of(w):
    rows = w.shape[0] // 2
    return lax.dynamic_slice_in_dim(w, lax.axis_index(C) * rows, rows, 0)


def split3(v):
    hi = lax.reduce_precision(v, 8, 7)
    mid = lax.reduce_precision(v - hi, 8, 7)
    return [hi, mid, v - hi - mid]


def from_peer(idx, d, q):
    core, p = idx[1], idx[2] ^ d
    z = ((q % (NZ // 2)) * 2 + (p & 1) + core) & (NZ - 1)
    y = ((q // (NZ // 2)) * 2 + (p >> 1) + core) & (NY - 1)
    return z * NY + y


def to_peer(idx, d, j, yh):
    core, p = idx[1], idx[2] ^ d
    zz = (p & 1) ^ core
    zh = (j - core * (1 - zz)) & (NZ // 2 - 1)
    y = (yh * 2 + (p >> 1) + core) & (NY - 1)
    return (2 * j + zz) * NY + y, yh * (NZ // 2) + zh


def matmuls(idx, xs, upv, dv, ov, outs, out_sems, wait_up, wait_down, nx):
    deep = xs.shape[1] // nx
    pre = None
    for k in range(nx):
        wait_up(k)
        rows = slice(k * deep, (k + 1) * deep)
        term = jnp.dot(xs[:, rows], upv[rows, :], preferred_element_type=F32)
        pre = term if pre is None else pre + term
    hidden = jnp.square(jnp.maximum(pre, 0.0)).astype(BF)
    half = hidden.shape[1] // 2
    copies = []
    wait_down()
    for j in range(nx):
        part = jnp.dot(hidden[:, :half], dv[2 * j], preferred_element_type=F32)
        part = part + jnp.dot(hidden[:, half:], dv[2 * j + 1], preferred_element_type=F32)
        part = part.astype(BF)
        for i in range(2 * NY):
            ov[2 * NY * j + i] = part[:, i * 128 : (i + 1) * 128]
        for d in range(4):
            for yh in range(NY // 2):
                slot, q = to_peer(idx, d, j, yh)
                sem = out_sems.at[(d * nx + j) * 2 + yh]
                copy = pltpu.make_async_copy(ov.at[slot], outs[d].at[q], sem)
                copy.start()
                copies.append(copy)
    for copy in copies:
        copy.wait()


def first_kernel(
    idx, x0, x1, x2, x3, up, own, m1, m2, m3, o1, o2, o3, u0, u1, u2, u3, xs, upv, dv, ov, x_sem, up_sem, d_sems, out_sems
):
    nx = dv.shape[0] // 2
    rows = dv.shape[1]
    me, core = idx[0], idx[1]
    x_copies = []
    for d, x in enumerate((x0, x1, x2, x3)):
        for q in range(x.shape[0]):
            at = pl.multiple_of(from_peer(idx, d, q) * 128, 128)
            copy = pltpu.make_async_copy(x.at[q], xs.at[:, pl.ds(at, 128)], x_sem.at[d * x.shape[0] + q])
            copy.start()
            x_copies.append(copy)
    deep = upv.shape[0] // nx
    up_copies = []
    for k in range(nx):
        chunk = pl.ds(k * deep, deep)
        up_copies.append(pltpu.make_async_copy(up.at[chunk], upv.at[chunk], up_sem.at[k]))
        up_copies[-1].start()
    d_copies = [
        pltpu.make_async_copy(own.at[pl.ds(0, rows)], dv.at[2 * me], d_sems.at[0]),
        pltpu.make_async_copy(own.at[pl.ds(rows, rows)], dv.at[2 * me + 1], d_sems.at[1]),
    ]
    for i, (by, mine, other) in enumerate(((1, m1, o1), (nx - 1, m2, o2), (2, m3, o3))):
        source = lax.rem(me + (nx - by), nx)
        d_copies.append(pltpu.make_async_copy(mine, dv.at[2 * source + core], d_sems.at[2 + 2 * i]))
        d_copies.append(pltpu.make_async_copy(other, dv.at[2 * source + 1 - core], d_sems.at[3 + 2 * i]))
    for copy in d_copies:
        copy.start()

    def wait_up(k):
        if k == 0:
            for copy in x_copies:
                copy.wait()
        up_copies[k].wait()

    def wait_down():
        for copy in d_copies:
            copy.wait()

    matmuls(idx, xs, upv, dv, ov, (u0, u1, u2, u3), out_sems, wait_up, wait_down, nx)


def second_kernel(
    idx, x0, x1, x2, x3, up, down, mixed, own_gain, own_bias, u0, u1, u2, u3, own, xs, xv, upv, dv, ov, gain, bias,
    x_sem, up_sem, d_sem, out_sems,
):
    nx = dv.shape[0] // 2
    nb = xv.shape[0]
    tokens = xs.shape[0]
    x_copies = []
    for d, x in enumerate((x0, x1, x2, x3)):
        for q in range(x.shape[0]):
            copy = pltpu.make_async_copy(x.at[q], xv.at[from_peer(idx, d, q)], x_sem.at[d * x.shape[0] + q])
            copy.start()
            x_copies.append(copy)
    up_copy = pltpu.make_async_copy(up, upv, up_sem)
    d_copy = pltpu.make_async_copy(down, dv, d_sem)
    up_copy.start()
    d_copy.start()
    for copy in x_copies:
        copy.wait()
    step = 64
    width = nb * 128
    for b in range(nb):
        t = xv[b, tokens : tokens + 8, :].astype(F32)
        gain[b : b + 1] = t[0:1] + t[1:2] + t[2:3]
        bias[b : b + 1] = t[3:4] + t[4:5] + t[5:6]

    def norm(i, carry):
        rows = pl.ds(pl.multiple_of(i * step, step), step)
        acc = jnp.zeros((step, 128), F32)
        for b in range(nb):
            acc = acc + xv[b, rows, :].astype(F32)
        mean = jnp.sum(acc, axis=1, keepdims=True) / width
        acc = jnp.zeros((step, 128), F32)
        for b in range(nb):
            d = xv[b, rows, :].astype(F32) - mean
            acc = acc + d * d
        scale = lax.rsqrt(jnp.sum(acc, axis=1, keepdims=True) / width + EPS)
        for b in range(nb):
            d = (xv[b, rows, :].astype(F32) - mean) * scale
            xs[rows, b * 128 : (b + 1) * 128] = (d * gain[b : b + 1] + bias[b : b + 1]).astype(BF)
        own[rows, :] = ((mixed[rows, :] - mean) * scale * own_gain[...] + own_bias[...]).astype(BF)
        return carry

    lax.fori_loop(0, tokens // step, norm, 0)

    def wait_up(k):
        if k == 0:
            up_copy.wait()

    matmuls(idx, xs, upv, dv, ov, (u0, u1, u2, u3), out_sems, wait_up, d_copy.wait, nx)


ANY = pl.BlockSpec(memory_space=pltpu.MemorySpace.HBM)
VMEM = pl.BlockSpec(memory_space=pltpu.MemorySpace.VMEM)
SMEM = pl.BlockSpec(memory_space=pltpu.MemorySpace.SMEM)


def first_ffn(idx, x, up, own, mine, others):
    tokens = x[0].shape[1]
    width, ff = up.shape
    nx, nb = lax.axis_size(X), NZ * NY
    return pl.pallas_call(
        first_kernel,
        out_shape=[jax.ShapeDtypeStruct((nb // 4, tokens, 128), BF)] * 4,
        in_specs=[SMEM] + [ANY] * 12,
        out_specs=[ANY] * 4,
        scratch_shapes=[
            pltpu.VMEM((tokens, width), BF),
            pltpu.VMEM((width, ff), BF),
            pltpu.VMEM((2 * nx, ff // 2, width // nx), BF),
            pltpu.VMEM((nb, tokens, 128), BF),
            pltpu.SemaphoreType.DMA((nb,)),
            pltpu.SemaphoreType.DMA((nx,)),
            pltpu.SemaphoreType.DMA((8,)),
            pltpu.SemaphoreType.DMA((nb,)),
        ],
        cost_estimate=pl.CostEstimate(flops=4 * tokens * width * ff, bytes_accessed=14 << 20, transcendentals=0),
        name="first_ffn",
    )(idx, *x, up, own, *mine, *others)


def second_ffn(idx, x, tokens, up, down, mixed, own_gain, own_bias):
    width, ff = up.shape
    nx, nb = lax.axis_size(X), NZ * NY
    return pl.pallas_call(
        second_kernel,
        out_shape=[jax.ShapeDtypeStruct((nb // 4, tokens, 128), BF)] * 4 + [jax.ShapeDtypeStruct((tokens, 128), BF)],
        in_specs=[SMEM] + [ANY] * 6 + [VMEM] * 3,
        out_specs=[ANY] * 4 + [VMEM],
        scratch_shapes=[
            pltpu.VMEM((tokens, width), BF),
            pltpu.VMEM((nb, *x[0].shape[1:]), BF),
            pltpu.VMEM((width, ff), BF),
            pltpu.VMEM((2 * nx, ff // 2, width // nx), BF),
            pltpu.VMEM((nb, tokens, 128), BF),
            pltpu.VMEM((nb, 128), F32),
            pltpu.VMEM((nb, 128), F32),
            pltpu.SemaphoreType.DMA((nb,)),
            pltpu.SemaphoreType.DMA,
            pltpu.SemaphoreType.DMA,
            pltpu.SemaphoreType.DMA((nb,)),
        ],
        cost_estimate=pl.CostEstimate(flops=4 * tokens * width * ff, bytes_accessed=14 << 20, transcendentals=0),
        name="second_ffn",
    )(idx, *x, up, down, mixed, own_gain, own_bias)


def body(
    stream,
    up_first,
    down_first,
    up_second,
    down_second,
    gain_first,
    bias_first,
    gain_second,
    bias_second,
):
    tokens = stream.shape[0]
    near, far = groups_of([lax.axis_size(axis) for axis in ALL])
    half = half_of(down_first)
    mine = [shift(half, X, by) for by in (1, -1, 2)]
    up_1 = lax.all_gather(half_of(up_first), (X, C), axis=0, tiled=True)
    x_far = far_to_all(stream, far)
    x_all = near_swap([x_far] * 4, near)
    others = [shift(m, C, 1) for m in mine]
    up_2 = lax.all_gather(half_of(up_second), (X, C), axis=0, tiled=True)
    down_2 = lax.all_gather(half_of(down_second), (X, C), axis=0, tiled=False)
    down_2 = down_2.reshape(-1, *half.shape)
    core = lax.axis_index(C)
    a, _ = place(lax.axis_index(Z), lax.axis_index(Y), core, NZ, NY)
    idx = jnp.stack([lax.axis_index(X), core, a]).astype(jnp.int32)
    parts = first_ffn(idx, x_all, up_1, down_first, mine, others)
    mixed = RESID * stream.astype(F32) + scattered_sum(parts, near, far)
    tail = jnp.stack(split3(gain_first) + split3(bias_first) + [jnp.zeros_like(gain_first)] * 2)
    mixed_all = gathered(jnp.concatenate([mixed, tail], axis=0).astype(BF), near, far)
    *parts, x = second_ffn(
        idx, mixed_all, tokens, up_2, down_2, mixed, gain_first[None], bias_first[None]
    )
    mixed = RESID * x.astype(F32) + scattered_sum(parts, near, far)
    width = mixed.shape[1] * lax.axis_size(RA)
    sums = jnp.concatenate([jnp.sum(mixed, axis=1), jnp.sum(mixed * mixed, axis=1)])
    sums = jnp.sum(stats_to_all(sums[None]), axis=0)[0]
    mean = sums[:tokens, None] / width
    var = sums[tokens:, None] / width - mean * mean
    return ((mixed - mean) * lax.rsqrt(var + EPS) * gain_second + bias_second).astype(BF)


def solution(mesh):
    torus = Mesh(mesh.devices.reshape(NZ, NY, mesh.shape["cb"], mesh.shape["dp"]), (Z, Y, X, C))
    in_specs = (
        P((X, C), RA),
        P(X, RA),
        P(RA, X),
        P(X, RA),
        P(RA, X),
        P(RA),
        P(RA),
        P(RA),
        P(RA),
    )
    out_specs = P((X, C), RA)

    return jax.shard_map(body, mesh=torus, in_specs=in_specs, out_specs=out_specs, check_vma=False)
```

```python
import jax
import jax.numpy as jnp
from jax import lax
from jax.experimental import pallas as pl
from jax.experimental.pallas import tpu as pltpu
from jax.sharding import Mesh
from jax.sharding import PartitionSpec as P


Z, Y, X, C = "ra_0", "ra_1", "cb", "dp"
RA = (Z, Y)
ALL = (Z, Y, X, C)
RESID = 1.4142135
EPS = 0.5
BF = jnp.bfloat16
F32 = jnp.float32
NZ, NY = 8, 4


def place(z, y, core):
    z, y = (z - core) % NZ, (y - core) % NY
    return (y % 2) * 2 + z % 2, y // 2, z // 2


def label(zh, p, core):
    return (zh - core * (1 - p % 2)) % (NZ // 2)


def pairs_of(sizes):
    nz, ny, nx, nc = sizes
    near, far = {}, {}
    for z in range(nz):
        for y in range(ny):
            for x in range(nx):
                for c in range(nc):
                    at = ((z * ny + y) * nx + x) * nc + c
                    p, yh, zh = place(z, y, c)
                    near.setdefault((x, c, yh, zh), {})[p] = at
                    far.setdefault((x, c, p), {})[yh * (nz // 2) + label(zh, p, c)] = at

    def flips(groups, by):
        return [(g[i], g[i ^ by]) for g in groups.values() for i in g]

    return {
        "near": [flips(near, d) for d in range(4)],
        "mid": [flips(far, (e >> 1) * (nz // 2) + (e & 1)) for e in range(4)],
        "last": flips(far, 2),
    }


def stage(blocks, pairs):
    own, diagonal, one, two = [blocks[0]] + [lax.ppermute(blocks[d], ALL, pairs[d]) for d in (3, 1, 2)]
    return [own, one, two, diagonal]


def gathered(pair, pairs):
    bundle = jnp.stack(stage([pair] * 4, pairs["mid"]))
    return stage([bundle] * 4, pairs["near"])


def scattered_sum(parts, pairs):
    some = sum(p.astype(F32) for p in stage(parts, pairs["near"])).astype(BF)
    return sum(p.astype(F32) for p in stage([some[e] for e in range(4)], pairs["mid"]))


def stats_to_all(row):
    n = lax.axis_size(RA)
    return lax.all_to_all(jnp.broadcast_to(row[None], (n, *row.shape)), RA, 0, 0, tiled=True)


def shift(a, axis, by):
    n = lax.axis_size(axis)
    return lax.ppermute(a, axis, [(i, (i + by) % n) for i in range(n)])


def half_of(w):
    rows = w.shape[0] // 2
    return lax.dynamic_slice_in_dim(w, lax.axis_index(C) * rows, rows, 0)


def split3(v):
    hi = lax.reduce_precision(v, 8, 7)
    mid = lax.reduce_precision(v - hi, 8, 7)
    return [hi, mid, v - hi - mid]


def from_peer(idx, d, e, g):
    core, p, yh, zh = idx[1], idx[2] ^ d, idx[3], idx[4]
    turn = core & (1 - (p & 1))
    zh = ((((zh - turn) & (NZ // 2 - 1)) ^ (g * 2 + (e & 1))) + turn) & (NZ // 2 - 1)
    z = (zh * 2 + (p & 1) + core) & (NZ - 1)
    y = ((yh ^ (e >> 1)) * 2 + (p >> 1) + core) & (NY - 1)
    return z * NY + y


def to_peer(idx, d, j, yh):
    core, p = idx[1], idx[2] ^ d
    turn = core & (1 - (p & 1))
    zz = (p & 1) ^ core
    zh = (j - core * (1 - zz)) & (NZ // 2 - 1)
    y = (yh * 2 + (p >> 1) + core) & (NY - 1)
    flip = ((zh - turn) & (NZ // 2 - 1)) ^ ((idx[4] - turn) & (NZ // 2 - 1))
    return (2 * j + zz) * NY + y, (flip & 1) + 2 * (yh ^ idx[3]), flip >> 1


def matmuls(idx, xs, upv, dv, ov, outs, out_sems, wait_up, wait_down, nx):
    deep = xs.shape[1] // nx
    pre = None
    for k in range(nx):
        wait_up(k)
        rows = slice(k * deep, (k + 1) * deep)
        term = jnp.dot(xs[:, rows], upv[rows, :], preferred_element_type=F32)
        pre = term if pre is None else pre + term
    hidden = jnp.square(jnp.maximum(pre, 0.0)).astype(BF)
    half = hidden.shape[1] // 2
    copies = []
    wait_down()
    for j in range(nx):
        part = jnp.dot(hidden[:, :half], dv[2 * j], preferred_element_type=F32)
        part = part + jnp.dot(hidden[:, half:], dv[2 * j + 1], preferred_element_type=F32)
        part = part.astype(BF)
        for i in range(2 * NY):
            ov[2 * NY * j + i] = part[:, i * 128 : (i + 1) * 128]
        for d in range(4):
            for yh in range(NY // 2):
                slot, e, g = to_peer(idx, d, j, yh)
                sem = out_sems.at[(d * nx + j) * 2 + yh]
                copy = pltpu.make_async_copy(ov.at[slot], outs[d].at[e, g], sem)
                copy.start()
                copies.append(copy)
    for copy in copies:
        copy.wait()


def first_kernel(
    idx, x0, x1, x2, x3, up, own, m1, m2, m3, o1, o2, o3, u0, u1, u2, u3, xs, upv, dv, ov, x_sem, up_sem, d_sems, out_sems
):
    nx = dv.shape[0] // 2
    rows = dv.shape[1]
    me, core = idx[0], idx[1]
    x_copies = []
    for d, x in enumerate((x0, x1, x2, x3)):
        for i in range(8):
            at = pl.multiple_of(from_peer(idx, d, i // 2, i % 2) * 128, 128)
            copy = pltpu.make_async_copy(x.at[i // 2, i % 2], xs.at[:, pl.ds(at, 128)], x_sem.at[d * 8 + i])
            copy.start()
            x_copies.append(copy)
    deep = upv.shape[0] // nx
    up_copies = []
    for k in range(nx):
        chunk = pl.ds(k * deep, deep)
        up_copies.append(pltpu.make_async_copy(up.at[chunk], upv.at[chunk], up_sem.at[k]))
        up_copies[-1].start()
    d_copies = [
        pltpu.make_async_copy(own.at[pl.ds(0, rows)], dv.at[2 * me], d_sems.at[0]),
        pltpu.make_async_copy(own.at[pl.ds(rows, rows)], dv.at[2 * me + 1], d_sems.at[1]),
    ]
    for i, (by, mine, other) in enumerate(((1, m1, o1), (nx - 1, m2, o2), (2, m3, o3))):
        source = lax.rem(me + (nx - by), nx)
        d_copies.append(pltpu.make_async_copy(mine, dv.at[2 * source + core], d_sems.at[2 + 2 * i]))
        d_copies.append(pltpu.make_async_copy(other, dv.at[2 * source + 1 - core], d_sems.at[3 + 2 * i]))
    for copy in d_copies:
        copy.start()

    def wait_up(k):
        if k == 0:
            for copy in x_copies:
                copy.wait()
        up_copies[k].wait()

    def wait_down():
        for copy in d_copies:
            copy.wait()

    matmuls(idx, xs, upv, dv, ov, (u0, u1, u2, u3), out_sems, wait_up, wait_down, nx)


def second_kernel(
    idx, x0, x1, x2, x3, up, down, mixed, own_gain, own_bias, u0, u1, u2, u3, own, xs, xv, upv, dv, ov, gain, bias,
    x_sem, up_sem, d_sem, out_sems,
):
    nx = dv.shape[0] // 2
    nb = xv.shape[0]
    tokens = xs.shape[0]
    x_copies = []
    for d, x in enumerate((x0, x1, x2, x3)):
        for i in range(8):
            to = xv.at[from_peer(idx, d, i // 2, i % 2)]
            copy = pltpu.make_async_copy(x.at[i // 2, i % 2], to, x_sem.at[d * 8 + i])
            copy.start()
            x_copies.append(copy)
    up_copy = pltpu.make_async_copy(up, upv, up_sem)
    d_copy = pltpu.make_async_copy(down, dv, d_sem)
    up_copy.start()
    d_copy.start()
    for copy in x_copies:
        copy.wait()
    step = 64
    width = nb * 128
    for b in range(nb):
        t = xv[b, tokens : tokens + 8, :].astype(F32)
        gain[b : b + 1] = t[0:1] + t[1:2] + t[2:3]
        bias[b : b + 1] = t[3:4] + t[4:5] + t[5:6]

    def norm(i, carry):
        rows = pl.ds(pl.multiple_of(i * step, step), step)
        acc = jnp.zeros((step, 128), F32)
        squares = jnp.zeros((step, 128), F32)
        for b in range(nb):
            d = xv[b, rows, :].astype(F32)
            acc = acc + d
            squares = squares + d * d
        mean = jnp.sum(acc, axis=1, keepdims=True) / width
        var = jnp.sum(squares, axis=1, keepdims=True) / width - mean * mean
        scale = lax.rsqrt(jnp.maximum(var, 0.0) + EPS)
        for b in range(nb):
            d = (xv[b, rows, :].astype(F32) - mean) * scale
            xs[rows, b * 128 : (b + 1) * 128] = (d * gain[b : b + 1] + bias[b : b + 1]).astype(BF)
        own[rows, :] = ((mixed[rows, :] - mean) * scale * own_gain[...] + own_bias[...]).astype(BF)
        return carry

    lax.fori_loop(0, tokens // step, norm, 0)

    def wait_up(k):
        if k == 0:
            up_copy.wait()

    matmuls(idx, xs, upv, dv, ov, (u0, u1, u2, u3), out_sems, wait_up, d_copy.wait, nx)


ANY = pl.BlockSpec(memory_space=pltpu.MemorySpace.HBM)
VMEM = pl.BlockSpec(memory_space=pltpu.MemorySpace.VMEM)
SMEM = pl.BlockSpec(memory_space=pltpu.MemorySpace.SMEM)


def first_ffn(idx, x, up, own, mine, others):
    tokens = x[0].shape[2]
    width, ff = up.shape
    nx, nb = lax.axis_size(X), NZ * NY
    return pl.pallas_call(
        first_kernel,
        out_shape=[jax.ShapeDtypeStruct((4, nb // 16, tokens, 128), BF)] * 4,
        in_specs=[SMEM] + [ANY] * 12,
        out_specs=[ANY] * 4,
        scratch_shapes=[
            pltpu.VMEM((tokens, width), BF),
            pltpu.VMEM((width, ff), BF),
            pltpu.VMEM((2 * nx, ff // 2, width // nx), BF),
            pltpu.VMEM((nb, tokens, 128), BF),
            pltpu.SemaphoreType.DMA((nb,)),
            pltpu.SemaphoreType.DMA((nx,)),
            pltpu.SemaphoreType.DMA((8,)),
            pltpu.SemaphoreType.DMA((nb,)),
        ],
        cost_estimate=pl.CostEstimate(flops=4 * tokens * width * ff, bytes_accessed=14 << 20, transcendentals=0),
        name="first_ffn",
    )(idx, *x, up, own, *mine, *others)


def second_ffn(idx, x, tokens, up, down, mixed, own_gain, own_bias):
    width, ff = up.shape
    nx, nb = lax.axis_size(X), NZ * NY
    return pl.pallas_call(
        second_kernel,
        out_shape=[jax.ShapeDtypeStruct((4, nb // 16, tokens, 128), BF)] * 4 + [jax.ShapeDtypeStruct((tokens, 128), BF)],
        in_specs=[SMEM] + [ANY] * 6 + [VMEM] * 3,
        out_specs=[ANY] * 4 + [VMEM],
        scratch_shapes=[
            pltpu.VMEM((tokens, width), BF),
            pltpu.VMEM((nb, *x[0].shape[2:]), BF),
            pltpu.VMEM((width, ff), BF),
            pltpu.VMEM((2 * nx, ff // 2, width // nx), BF),
            pltpu.VMEM((nb, tokens, 128), BF),
            pltpu.VMEM((nb, 128), F32),
            pltpu.VMEM((nb, 128), F32),
            pltpu.SemaphoreType.DMA((nb,)),
            pltpu.SemaphoreType.DMA,
            pltpu.SemaphoreType.DMA,
            pltpu.SemaphoreType.DMA((nb,)),
        ],
        cost_estimate=pl.CostEstimate(flops=4 * tokens * width * ff, bytes_accessed=14 << 20, transcendentals=0),
        name="second_ffn",
    )(idx, *x, up, down, mixed, own_gain, own_bias)


def body(
    stream,
    up_first,
    down_first,
    up_second,
    down_second,
    gain_first,
    bias_first,
    gain_second,
    bias_second,
):
    tokens = stream.shape[0]
    pairs = pairs_of([lax.axis_size(axis) for axis in ALL])
    pair = jnp.stack([stream, lax.ppermute(stream, ALL, pairs["last"])])
    half = half_of(down_first)
    mine = [shift(half, X, by) for by in (1, -1, 2)]
    up_1 = lax.all_gather(half_of(up_first), (X, C), axis=0, tiled=True)
    x_all = gathered(pair, pairs)
    others = [shift(m, C, 1) for m in mine]
    up_2 = lax.all_gather(half_of(up_second), (X, C), axis=0, tiled=True)
    down_2 = lax.all_gather(half_of(down_second), (X, C), axis=0, tiled=False)
    down_2 = down_2.reshape(-1, *half.shape)
    core = lax.axis_index(C)
    p, yh, zh = place(lax.axis_index(Z), lax.axis_index(Y), core)
    idx = jnp.stack([lax.axis_index(X), core, p, yh, zh]).astype(jnp.int32)
    parts = first_ffn(idx, x_all, up_1, down_first, mine, others)
    tail = jnp.stack(split3(gain_first) + split3(bias_first) + [jnp.zeros_like(gain_first)] * 2).astype(BF)
    tails = jnp.stack([tail, lax.ppermute(tail, ALL, pairs["last"])])
    some = scattered_sum(parts, pairs).astype(BF)
    branch = some.astype(F32) + lax.ppermute(some, ALL, pairs["last"])[::-1].astype(F32)
    mixed = RESID * pair.astype(F32) + branch
    mixed_all = gathered(jnp.concatenate([mixed.astype(BF), tails], axis=1), pairs)
    *parts, x = second_ffn(
        idx, mixed_all, tokens, up_2, down_2, mixed[0], gain_first[None], bias_first[None]
    )
    some = scattered_sum(parts, pairs)
    branch = some[0] + lax.ppermute(some[1].astype(BF), ALL, pairs["last"]).astype(F32)
    mixed = RESID * x.astype(F32) + branch
    width = mixed.shape[1] * lax.axis_size(RA)
    sums = jnp.concatenate([jnp.sum(mixed, axis=1), jnp.sum(mixed * mixed, axis=1)])
    sums = jnp.sum(stats_to_all(sums[None]), axis=0)[0]
    mean = sums[:tokens, None] / width
    var = sums[tokens:, None] / width - mean * mean
    return ((mixed - mean) * lax.rsqrt(var + EPS) * gain_second + bias_second).astype(BF)


def solution(mesh):
    torus = Mesh(mesh.devices.reshape(NZ, NY, mesh.shape["cb"], mesh.shape["dp"]), (Z, Y, X, C))
    in_specs = (
        P((X, C), RA),
        P(X, RA),
        P(RA, X),
        P(X, RA),
        P(RA, X),
        P(RA),
        P(RA),
        P(RA),
        P(RA),
    )
    out_specs = P((X, C), RA)

    return jax.shard_map(body, mesh=torus, in_specs=in_specs, out_specs=out_specs, check_vma=False)
```

```python
import jax
import jax.numpy as jnp
from jax import lax
from jax.experimental import pallas as pl
from jax.experimental.pallas import tpu as pltpu
from jax.sharding import Mesh
from jax.sharding import PartitionSpec as P


Z, Y, X, C = "ra_0", "ra_1", "cb", "dp"
RA = (Z, Y)
ALL = (Z, Y, X, C)
RESID = 1.4142135
EPS = 0.5
BF = jnp.bfloat16
F32 = jnp.float32
NZ, NY = 8, 4


def place(z, y, core):
    z, y = (z - core) % NZ, (y - core) % NY
    return (y % 2) * 2 + z % 2, y // 2, z // 2


def label(zh, p, core):
    return (zh - core * (1 - p % 2)) % (NZ // 2)


def pairs_of(sizes):
    nz, ny, nx, nc = sizes
    near, far = {}, {}
    for z in range(nz):
        for y in range(ny):
            for x in range(nx):
                for c in range(nc):
                    at = ((z * ny + y) * nx + x) * nc + c
                    p, yh, zh = place(z, y, c)
                    near.setdefault((x, c, yh, zh), {})[p] = at
                    far.setdefault((x, c, p), {})[yh * (nz // 2) + label(zh, p, c)] = at

    def flips(groups, by):
        return [(g[i], g[i ^ by]) for g in groups.values() for i in g]

    return {
        "near": [flips(near, d) for d in range(4)],
        "mid": [flips(far, (e >> 1) * (nz // 2) + (e & 1)) for e in range(4)],
        "last": flips(far, 2),
    }


def stage(blocks, pairs):
    own, diagonal, one, two = [blocks[0]] + [lax.ppermute(blocks[d], ALL, pairs[d]) for d in (3, 1, 2)]
    return [own, one, two, diagonal]


def gathered(pair, pairs):
    bundle = jnp.stack(stage([pair] * 4, pairs["mid"]))
    return stage([bundle] * 4, pairs["near"])


def scattered_sum(parts, pairs):
    some = sum(p.astype(F32) for p in stage(parts, pairs["near"])).astype(BF)
    return sum(p.astype(F32) for p in stage([some[e] for e in range(4)], pairs["mid"]))


def stats_to_all(row):
    n = lax.axis_size(RA)
    return lax.all_to_all(jnp.broadcast_to(row[None], (n, *row.shape)), RA, 0, 0, tiled=True)


def shift(a, axis, by):
    n = lax.axis_size(axis)
    return lax.ppermute(a, axis, [(i, (i + by) % n) for i in range(n)])


def half_of(w):
    rows = w.shape[0] // 2
    return lax.dynamic_slice_in_dim(w, lax.axis_index(C) * rows, rows, 0)


def packed(up, down):
    up, down = half_of(up), half_of(down)
    width = up.shape[1]
    return jnp.concatenate([up] + [down[:, i : i + width] for i in range(0, down.shape[1], width)], axis=0)


def split3(v):
    hi = lax.reduce_precision(v, 8, 7)
    mid = lax.reduce_precision(v - hi, 8, 7)
    return [hi, mid, v - hi - mid]


def from_peer(idx, d, e, g):
    core, p, yh, zh = idx[1], idx[2] ^ d, idx[3], idx[4]
    turn = core & (1 - (p & 1))
    zh = ((((zh - turn) & (NZ // 2 - 1)) ^ (g * 2 + (e & 1))) + turn) & (NZ // 2 - 1)
    z = (zh * 2 + (p & 1) + core) & (NZ - 1)
    y = ((yh ^ (e >> 1)) * 2 + (p >> 1) + core) & (NY - 1)
    return z * NY + y


def to_peer(idx, d, j, yh):
    core, p = idx[1], idx[2] ^ d
    turn = core & (1 - (p & 1))
    zz = (p & 1) ^ core
    zh = (j - core * (1 - zz)) & (NZ // 2 - 1)
    y = (yh * 2 + (p >> 1) + core) & (NY - 1)
    flip = ((zh - turn) & (NZ // 2 - 1)) ^ ((idx[4] - turn) & (NZ // 2 - 1))
    return (2 * j + zz) * NY + y, (flip & 1) + 2 * (yh ^ idx[3]), flip >> 1


def matmuls(idx, xs, upv, dv, ov, outs, out_sems, before_up, before_down):
    nx = dv.shape[0] // 2
    for copy in before_up:
        copy.wait()
    pre = jnp.dot(xs[...], upv[...], preferred_element_type=F32)
    hidden = jnp.square(jnp.maximum(pre, 0.0)).astype(BF)
    half = hidden.shape[1] // 2
    copies = []
    for copy in before_down:
        copy.wait()
    for j in range(nx):
        part = jnp.dot(hidden[:, :half], dv[2 * j], preferred_element_type=F32)
        part = part + jnp.dot(hidden[:, half:], dv[2 * j + 1], preferred_element_type=F32)
        part = part.astype(BF)
        for i in range(2 * NY):
            ov[2 * NY * j + i] = part[:, i * 128 : (i + 1) * 128]
        for d in range(4):
            for yh in range(NY // 2):
                slot, e, g = to_peer(idx, d, j, yh)
                sem = out_sems.at[(d * nx + j) * 2 + yh]
                copy = pltpu.make_async_copy(ov.at[slot], outs[d].at[e, g], sem)
                copy.start()
                copies.append(copy)
    for copy in copies:
        copy.wait()


def load_weights(idx, up, down, pieces, upv, dv, up_sems, d_sems):
    nx = dv.shape[0] // 2
    rows, wide = dv.shape[1:]
    width = upv.shape[1]
    deep = upv.shape[0] // nx
    me, core = idx[0], idx[1]

    def up_rows(source, half, count):
        return upv.at[pl.ds(pl.multiple_of(source * deep + half * (deep // 2), deep // 2), count)]

    ups = [pltpu.make_async_copy(up, up_rows(me, 0, deep), up_sems.at[0])]
    downs = [pltpu.make_async_copy(down.at[pl.ds(i * rows, rows)], dv.at[2 * me + i], d_sems.at[i]) for i in range(2)]
    for i, piece in enumerate(pieces):
        by = (1, nx - 1, 2)[i % 3]
        source = lax.rem(me + (nx - by), nx)
        half = core if i < 3 else 1 - core
        ups.append(
            pltpu.make_async_copy(piece.at[pl.ds(0, deep // 2)], up_rows(source, half, deep // 2), up_sems.at[1 + i])
        )
        for k in range(wide // width):
            downs.append(
                pltpu.make_async_copy(
                    piece.at[pl.ds(deep // 2 + k * rows, rows)],
                    dv.at[2 * source + half, :, pl.ds(k * width, width)],
                    d_sems.at[2 + 2 * i + k],
                )
            )
    for copy in ups + downs:
        copy.start()
    return ups, downs


def first_kernel(
    idx, x0, x1, x2, x3, up, down, m1, m2, m3, o1, o2, o3, u0, u1, u2, u3, xs, upv, dv, ov, x_sem, up_sems, d_sems, out_sems
):
    x_copies = []
    for d, x in enumerate((x0, x1, x2, x3)):
        for i in range(8):
            at = pl.multiple_of(from_peer(idx, d, i // 2, i % 2) * 128, 128)
            copy = pltpu.make_async_copy(x.at[i // 2, i % 2], xs.at[:, pl.ds(at, 128)], x_sem.at[d * 8 + i])
            copy.start()
            x_copies.append(copy)
    ups, downs = load_weights(idx, up, down, (m1, m2, m3, o1, o2, o3), upv, dv, up_sems, d_sems)
    matmuls(idx, xs, upv, dv, ov, (u0, u1, u2, u3), out_sems, x_copies + ups, downs)


def second_kernel(
    idx, x0, x1, x2, x3, up, down, m1, m2, m3, o1, o2, o3, mixed, own_gain, own_bias, u0, u1, u2, u3, own,
    xs, xv, upv, dv, ov, gain, bias, x_sem, up_sems, d_sems, out_sems,
):
    nb = xv.shape[0]
    tokens = xs.shape[0]
    x_copies = []
    for d, x in enumerate((x0, x1, x2, x3)):
        for i in range(8):
            to = xv.at[from_peer(idx, d, i // 2, i % 2)]
            copy = pltpu.make_async_copy(x.at[i // 2, i % 2], to, x_sem.at[d * 8 + i])
            copy.start()
            x_copies.append(copy)
    ups, downs = load_weights(idx, up, down, (m1, m2, m3, o1, o2, o3), upv, dv, up_sems, d_sems)
    for copy in x_copies:
        copy.wait()
    step = 64
    width = nb * 128
    for b in range(nb):
        t = xv[b, tokens : tokens + 8, :].astype(F32)
        gain[b : b + 1] = t[0:1] + t[1:2] + t[2:3]
        bias[b : b + 1] = t[3:4] + t[4:5] + t[5:6]

    def norm(i, carry):
        rows = pl.ds(pl.multiple_of(i * step, step), step)
        acc = jnp.zeros((step, 128), F32)
        squares = jnp.zeros((step, 128), F32)
        for b in range(nb):
            d = xv[b, rows, :].astype(F32)
            acc = acc + d
            squares = squares + d * d
        mean = jnp.sum(acc, axis=1, keepdims=True) / width
        var = jnp.sum(squares, axis=1, keepdims=True) / width - mean * mean
        scale = lax.rsqrt(jnp.maximum(var, 0.0) + EPS)
        for b in range(nb):
            d = (xv[b, rows, :].astype(F32) - mean) * scale
            xs[rows, b * 128 : (b + 1) * 128] = (d * gain[b : b + 1] + bias[b : b + 1]).astype(BF)
        own[rows, :] = ((mixed[rows, :] - mean) * scale * own_gain[...] + own_bias[...]).astype(BF)
        return carry

    lax.fori_loop(0, tokens // step, norm, 0)

    matmuls(idx, xs, upv, dv, ov, (u0, u1, u2, u3), out_sems, ups, downs)


ANY = pl.BlockSpec(memory_space=pltpu.MemorySpace.HBM)
VMEM = pl.BlockSpec(memory_space=pltpu.MemorySpace.VMEM)
SMEM = pl.BlockSpec(memory_space=pltpu.MemorySpace.SMEM)


def ffn(kernel, idx, x, tokens, up, down, pieces, extra, own_out, norm_scratch):
    nx, nb = lax.axis_size(X), NZ * NY
    width, ff = up.shape[0] * nx, up.shape[1]
    return pl.pallas_call(
        kernel,
        out_shape=[jax.ShapeDtypeStruct((4, nb // 16, tokens, 128), BF)] * 4 + own_out,
        in_specs=[SMEM] + [ANY] * (6 + len(pieces)) + [VMEM] * len(extra),
        out_specs=[ANY] * 4 + [VMEM] * len(own_out),
        scratch_shapes=[pltpu.VMEM((tokens, width), BF)]
        + norm_scratch[:1]
        + [
            pltpu.VMEM((width, ff), BF),
            pltpu.VMEM((2 * nx, ff // 2, width // nx), BF),
            pltpu.VMEM((nb, tokens, 128), BF),
        ]
        + norm_scratch[1:]
        + [
            pltpu.SemaphoreType.DMA((nb,)),
            pltpu.SemaphoreType.DMA((7,)),
            pltpu.SemaphoreType.DMA((14,)),
            pltpu.SemaphoreType.DMA((nb,)),
        ],
        cost_estimate=pl.CostEstimate(flops=4 * tokens * width * ff, bytes_accessed=14 << 20, transcendentals=0),
    )(idx, *x, up, down, *pieces, *extra)


def body(
    stream,
    up_first,
    down_first,
    up_second,
    down_second,
    gain_first,
    bias_first,
    gain_second,
    bias_second,
):
    tokens = stream.shape[0]
    pairs = pairs_of([lax.axis_size(axis) for axis in ALL])
    pair = jnp.stack([stream, lax.ppermute(stream, ALL, pairs["last"])])
    w = packed(up_first, down_first)
    mine_1 = [shift(w, X, by) for by in (1, -1, 2)]
    x_all = gathered(pair, pairs)
    others_1 = [shift(m, C, 1) for m in mine_1]
    w = packed(up_second, down_second)
    mine_2 = [shift(w, X, by) for by in (1, -1, 2)]
    core = lax.axis_index(C)
    p, yh, zh = place(lax.axis_index(Z), lax.axis_index(Y), core)
    idx = jnp.stack([lax.axis_index(X), core, p, yh, zh]).astype(jnp.int32)
    parts = ffn(first_kernel, idx, x_all, tokens, up_first, down_first, mine_1 + others_1, [], [], [])
    tail = jnp.stack(split3(gain_first) + split3(bias_first) + [jnp.zeros_like(gain_first)] * 2).astype(BF)
    tails = jnp.broadcast_to(tail[None], (2, *tail.shape))
    some = jnp.concatenate([scattered_sum(parts, pairs).astype(BF), tails], axis=1)
    there = lax.ppermute(some, ALL, pairs["last"])[::-1]
    mixed = RESID * pair.astype(F32) + some[:, :tokens].astype(F32) + there[:, :tokens].astype(F32)
    tails = jnp.stack([tail, there[1, tokens:]])
    mixed_all = gathered(jnp.concatenate([mixed.astype(BF), tails], axis=1), pairs)
    others_2 = [shift(m, C, 1) for m in mine_2]
    nb = NZ * NY
    *parts, x = ffn(
        second_kernel, idx, mixed_all, tokens, up_second, down_second, mine_2 + others_2,
        [mixed[0], gain_first[None], bias_first[None]],
        [jax.ShapeDtypeStruct((tokens, 128), BF)],
        [pltpu.VMEM((nb, tokens + 8, 128), BF), pltpu.VMEM((nb, 128), F32), pltpu.VMEM((nb, 128), F32)],
    )
    some = scattered_sum(parts, pairs)
    branch = some[0] + lax.ppermute(some[1].astype(BF), ALL, pairs["last"]).astype(F32)
    mixed = RESID * x.astype(F32) + branch
    width = mixed.shape[1] * lax.axis_size(RA)
    sums = jnp.concatenate([jnp.sum(mixed, axis=1), jnp.sum(mixed * mixed, axis=1)])
    sums = jnp.sum(stats_to_all(sums[None]), axis=0)[0]
    mean = sums[:tokens, None] / width
    var = sums[tokens:, None] / width - mean * mean
    return ((mixed - mean) * lax.rsqrt(var + EPS) * gain_second + bias_second).astype(BF)


def solution(mesh):
    torus = Mesh(mesh.devices.reshape(NZ, NY, mesh.shape["cb"], mesh.shape["dp"]), (Z, Y, X, C))
    in_specs = (
        P((X, C), RA),
        P(X, RA),
        P(RA, X),
        P(X, RA),
        P(RA, X),
        P(RA),
        P(RA),
        P(RA),
        P(RA),
    )
    out_specs = P((X, C), RA)

    return jax.shard_map(body, mesh=torus, in_specs=in_specs, out_specs=out_specs, check_vma=False)
```

```python
import jax
import jax.numpy as jnp
from jax import lax
from jax.experimental import pallas as pl
from jax.experimental.pallas import tpu as pltpu
from jax.sharding import Mesh
from jax.sharding import PartitionSpec as P


Z, Y, X, C = "ra_0", "ra_1", "cb", "dp"
RA = (Z, Y)
ALL = (Z, Y, X, C)
RESID = 1.4142135
EPS = 0.5
BF = jnp.bfloat16
F32 = jnp.float32
NZ, NY = 8, 4


def place(z, y, core):
    z, y = (z - core) % NZ, (y - core) % NY
    return (y % 2) * 2 + z % 2, y // 2, z // 2


def label(zh, p, core):
    return (zh - core * (1 - p % 2)) % (NZ // 2)


def pairs_of(sizes):
    nz, ny, nx, nc = sizes
    near, far = {}, {}
    for z in range(nz):
        for y in range(ny):
            for x in range(nx):
                for c in range(nc):
                    at = ((z * ny + y) * nx + x) * nc + c
                    p, yh, zh = place(z, y, c)
                    near.setdefault((x, c, yh, zh), {})[p] = at
                    far.setdefault((x, c, p), {})[yh * (nz // 2) + label(zh, p, c)] = at

    def flips(groups, by):
        return [(g[i], g[i ^ by]) for g in groups.values() for i in g]

    return {
        "near": [flips(near, d) for d in range(4)],
        "mid": [flips(far, (e >> 1) * (nz // 2) + (e & 1)) for e in range(4)],
        "last": flips(far, 2),
    }


def stage(blocks, pairs):
    got = {d: lax.ppermute(blocks[d], ALL, pairs[d]) for d in (1, 2, 3)}
    own, diagonal, one, two = blocks[0], got[3], got[1], got[2]
    return [own, one, two, diagonal]


def gathered(pair, pairs):
    bundle = jnp.stack(stage([pair] * 4, pairs["mid"]))
    return stage([bundle] * 4, pairs["near"])


def scattered_sum(parts, pairs):
    some = sum(p.astype(F32) for p in stage(parts, pairs["near"])).astype(BF)
    return sum(p.astype(F32) for p in stage([some[e] for e in range(4)], pairs["mid"]))


def stats_to_all(row):
    n = lax.axis_size(RA)
    return lax.all_to_all(jnp.broadcast_to(row[None], (n, *row.shape)), RA, 0, 0, tiled=True)


def shift(a, axis, by):
    n = lax.axis_size(axis)
    return lax.ppermute(a, axis, [(i, (i + by) % n) for i in range(n)])


def half_of(w):
    rows = w.shape[0] // 2
    return lax.dynamic_slice_in_dim(w, lax.axis_index(C) * rows, rows, 0)


def packed(up, down):
    up, down = half_of(up), half_of(down)
    width = up.shape[1]
    return jnp.concatenate([up] + [down[:, i : i + width] for i in range(0, down.shape[1], width)], axis=0)


def split3(v):
    hi = lax.reduce_precision(v, 8, 7)
    mid = lax.reduce_precision(v - hi, 8, 7)
    return [hi, mid, v - hi - mid]


def from_peer(idx, d, e, g):
    core, p, yh, zh = idx[1], idx[2] ^ d, idx[3], idx[4]
    turn = core & (1 - (p & 1))
    zh = ((((zh - turn) & (NZ // 2 - 1)) ^ (g * 2 + (e & 1))) + turn) & (NZ // 2 - 1)
    z = (zh * 2 + (p & 1) + core) & (NZ - 1)
    y = ((yh ^ (e >> 1)) * 2 + (p >> 1) + core) & (NY - 1)
    return z * NY + y


def to_peer(idx, d, j, yh):
    core, p = idx[1], idx[2] ^ d
    turn = core & (1 - (p & 1))
    zz = (p & 1) ^ core
    zh = (j - core * (1 - zz)) & (NZ // 2 - 1)
    y = (yh * 2 + (p >> 1) + core) & (NY - 1)
    flip = ((zh - turn) & (NZ // 2 - 1)) ^ ((idx[4] - turn) & (NZ // 2 - 1))
    return (2 * j + zz) * NY + y, (flip & 1) + 2 * (yh ^ idx[3]), flip >> 1


def matmuls(idx, xs, upv, dv, ov, outs, out_sems, before_up, before_down):
    nx = dv.shape[0] // 2
    for copy in before_up:
        copy.wait()
    pre = jnp.dot(xs[...], upv[...], preferred_element_type=F32)
    hidden = jnp.square(jnp.maximum(pre, 0.0)).astype(BF)
    half = hidden.shape[1] // 2
    copies = []
    for copy in before_down:
        copy.wait()
    for j in range(nx):
        part = jnp.dot(hidden[:, :half], dv[2 * j], preferred_element_type=F32)
        part = part + jnp.dot(hidden[:, half:], dv[2 * j + 1], preferred_element_type=F32)
        part = part.astype(BF)
        for i in range(2 * NY):
            ov[2 * NY * j + i] = part[:, i * 128 : (i + 1) * 128]
        for d in range(4):
            for yh in range(NY // 2):
                slot, e, g = to_peer(idx, d, j, yh)
                sem = out_sems.at[(d * nx + j) * 2 + yh]
                copy = pltpu.make_async_copy(ov.at[slot], outs[d].at[e, g], sem)
                copy.start()
                copies.append(copy)
    for copy in copies:
        copy.wait()


def load_weights(idx, up, down, pieces, upv, dv, up_sems, d_sems):
    nx = dv.shape[0] // 2
    rows, wide = dv.shape[1:]
    width = upv.shape[1]
    deep = upv.shape[0] // nx
    me, core = idx[0], idx[1]

    def up_rows(source, half, count):
        return upv.at[pl.ds(pl.multiple_of(source * deep + half * (deep // 2), deep // 2), count)]

    ups = [pltpu.make_async_copy(up, up_rows(me, 0, deep), up_sems.at[0])]
    downs = [pltpu.make_async_copy(down.at[pl.ds(i * rows, rows)], dv.at[2 * me + i], d_sems.at[i]) for i in range(2)]
    for i, (piece, by, same) in enumerate(pieces):
        source = lax.rem(me + (nx - by), nx)
        half = core if same else 1 - core
        if not isinstance(piece, tuple):
            piece = (piece.at[pl.ds(0, deep // 2)], piece.at[pl.ds(deep // 2, deep // 2)])
        ups.append(pltpu.make_async_copy(piece[0], up_rows(source, half, deep // 2), up_sems.at[1 + i]))
        for k in range(wide // width):
            downs.append(
                pltpu.make_async_copy(
                    piece[1].at[pl.ds(k * rows, rows)],
                    dv.at[2 * source + half, :, pl.ds(k * width, width)],
                    d_sems.at[2 + 2 * i + k],
                )
            )
    for copy in ups + downs:
        copy.start()
    return ups, downs


def first_kernel(
    idx, x0, x1, x2, x3, up, down, m1, m3, fu, fd, o1, o3, pu, pd, u0, u1, u2, u3, xs, upv, dv, ov, x_sem, up_sems, d_sems, out_sems
):
    x_copies = []
    for d, x in enumerate((x0, x1, x2, x3)):
        for i in range(8):
            at = pl.multiple_of(from_peer(idx, d, i // 2, i % 2) * 128, 128)
            copy = pltpu.make_async_copy(x.at[i // 2, i % 2], xs.at[:, pl.ds(at, 128)], x_sem.at[d * 8 + i])
            copy.start()
            x_copies.append(copy)
    pieces = [(m1, 1, True), (m3, 3, True), ((fu, fd), 2, True), (o1, 1, False), (o3, 3, False), ((pu, pd), 2, False)]
    ups, downs = load_weights(idx, up, down, pieces, upv, dv, up_sems, d_sems)
    matmuls(idx, xs, upv, dv, ov, (u0, u1, u2, u3), out_sems, x_copies + ups, downs)


def second_kernel(
    idx, x0, x1, x2, x3, up, down, m1, m2, m3, o1, o2, o3, mixed, own_gain, own_bias, u0, u1, u2, u3, own,
    xs, xv, upv, dv, ov, gain, bias, x_sem, up_sems, d_sems, out_sems,
):
    nb = xv.shape[0]
    tokens = xs.shape[0]
    x_copies = []
    for d, x in enumerate((x0, x1, x2, x3)):
        for i in range(8):
            to = xv.at[from_peer(idx, d, i // 2, i % 2)]
            copy = pltpu.make_async_copy(x.at[i // 2, i % 2], to, x_sem.at[d * 8 + i])
            copy.start()
            x_copies.append(copy)
    pieces = [(m1, 1, True), (m2, 3, True), (m3, 2, True), (o1, 1, False), (o2, 3, False), (o3, 2, False)]
    ups, downs = load_weights(idx, up, down, pieces, upv, dv, up_sems, d_sems)
    for copy in x_copies:
        copy.wait()
    step = 64
    width = nb * 128
    for b in range(nb):
        t = xv[b, tokens : tokens + 8, :].astype(F32)
        gain[b : b + 1] = t[0:1] + t[1:2] + t[2:3]
        bias[b : b + 1] = t[3:4] + t[4:5] + t[5:6]

    def norm(i, carry):
        rows = pl.ds(pl.multiple_of(i * step, step), step)
        acc = jnp.zeros((step, 128), F32)
        squares = jnp.zeros((step, 128), F32)
        for b in range(nb):
            d = xv[b, rows, :].astype(F32)
            acc = acc + d
            squares = squares + d * d
        mean = jnp.sum(acc, axis=1, keepdims=True) / width
        var = jnp.sum(squares, axis=1, keepdims=True) / width - mean * mean
        scale = lax.rsqrt(jnp.maximum(var, 0.0) + EPS)
        for b in range(nb):
            d = (xv[b, rows, :].astype(F32) - mean) * scale
            xs[rows, b * 128 : (b + 1) * 128] = (d * gain[b : b + 1] + bias[b : b + 1]).astype(BF)
        own[rows, :] = ((mixed[rows, :] - mean) * scale * own_gain[...] + own_bias[...]).astype(BF)
        return carry

    lax.fori_loop(0, tokens // step, norm, 0)

    matmuls(idx, xs, upv, dv, ov, (u0, u1, u2, u3), out_sems, ups, downs)


ANY = pl.BlockSpec(memory_space=pltpu.MemorySpace.HBM)
VMEM = pl.BlockSpec(memory_space=pltpu.MemorySpace.VMEM)
SMEM = pl.BlockSpec(memory_space=pltpu.MemorySpace.SMEM)


def ffn(kernel, idx, x, tokens, up, down, pieces, extra, own_out, norm_scratch):
    nx, nb = lax.axis_size(X), NZ * NY
    width, ff = up.shape[0] * nx, up.shape[1]
    return pl.pallas_call(
        kernel,
        out_shape=[jax.ShapeDtypeStruct((4, nb // 16, tokens, 128), BF)] * 4 + own_out,
        in_specs=[SMEM] + [ANY] * (6 + len(pieces)) + [VMEM] * len(extra),
        out_specs=[ANY] * 4 + [VMEM] * len(own_out),
        scratch_shapes=[pltpu.VMEM((tokens, width), BF)]
        + norm_scratch[:1]
        + [
            pltpu.VMEM((width, ff), BF),
            pltpu.VMEM((2 * nx, ff // 2, width // nx), BF),
            pltpu.VMEM((nb, tokens, 128), BF),
        ]
        + norm_scratch[1:]
        + [
            pltpu.SemaphoreType.DMA((nb,)),
            pltpu.SemaphoreType.DMA((7,)),
            pltpu.SemaphoreType.DMA((14,)),
            pltpu.SemaphoreType.DMA((nb,)),
        ],
        cost_estimate=pl.CostEstimate(flops=4 * tokens * width * ff, bytes_accessed=14 << 20, transcendentals=0),
    )(idx, *x, up, down, *pieces, *extra)


def body(
    stream,
    up_first,
    down_first,
    up_second,
    down_second,
    gain_first,
    bias_first,
    gain_second,
    bias_second,
):
    tokens = stream.shape[0]
    pairs = pairs_of([lax.axis_size(axis) for axis in ALL])
    pair = jnp.stack([stream, lax.ppermute(stream, ALL, pairs["last"])])
    w = packed(up_first, down_first)
    left, right = shift(w, X, 1), shift(w, X, -1)
    x_all = gathered(pair, pairs)
    cut = w.shape[0] // 2
    mine_1 = [left, right, shift(left[:cut], X, 1), shift(right[cut:], X, -1)]
    others_1 = [shift(m, C, 1) for m in mine_1]
    w = packed(up_second, down_second)
    mine_2 = [shift(w, X, by) for by in (1, -1, 2)]
    core = lax.axis_index(C)
    p, yh, zh = place(lax.axis_index(Z), lax.axis_index(Y), core)
    idx = jnp.stack([lax.axis_index(X), core, p, yh, zh]).astype(jnp.int32)
    parts = ffn(first_kernel, idx, x_all, tokens, up_first, down_first, mine_1 + others_1, [], [], [])
    tail = jnp.stack(split3(gain_first) + split3(bias_first) + [jnp.zeros_like(gain_first)] * 2).astype(BF)
    tails = jnp.broadcast_to(tail[None], (2, *tail.shape))
    some = jnp.concatenate([scattered_sum(parts, pairs).astype(BF), tails], axis=1)
    there = lax.ppermute(some, ALL, pairs["last"])[::-1]
    mixed = RESID * pair.astype(F32) + some[:, :tokens].astype(F32) + there[:, :tokens].astype(F32)
    tails = jnp.stack([tail, there[1, tokens:]])
    mixed_all = gathered(jnp.concatenate([mixed.astype(BF), tails], axis=1), pairs)
    others_2 = [shift(m, C, 1) for m in mine_2]
    nb = NZ * NY
    *parts, x = ffn(
        second_kernel, idx, mixed_all, tokens, up_second, down_second, mine_2 + others_2,
        [mixed[0], gain_first[None], bias_first[None]],
        [jax.ShapeDtypeStruct((tokens, 128), BF)],
        [pltpu.VMEM((nb, tokens + 8, 128), BF), pltpu.VMEM((nb, 128), F32), pltpu.VMEM((nb, 128), F32)],
    )
    some = scattered_sum(parts, pairs)
    branch = some[0] + lax.ppermute(some[1].astype(BF), ALL, pairs["last"]).astype(F32)
    mixed = RESID * x.astype(F32) + branch
    width = mixed.shape[1] * lax.axis_size(RA)
    sums = jnp.concatenate([jnp.sum(mixed, axis=1), jnp.sum(mixed * mixed, axis=1)])
    sums = jnp.sum(stats_to_all(sums[None]), axis=0)[0]
    mean = sums[:tokens, None] / width
    var = sums[tokens:, None] / width - mean * mean
    return ((mixed - mean) * lax.rsqrt(var + EPS) * gain_second + bias_second).astype(BF)


def solution(mesh):
    torus = Mesh(mesh.devices.reshape(NZ, NY, mesh.shape["cb"], mesh.shape["dp"]), (Z, Y, X, C))
    in_specs = (
        P((X, C), RA),
        P(X, RA),
        P(RA, X),
        P(X, RA),
        P(RA, X),
        P(RA),
        P(RA),
        P(RA),
        P(RA),
    )
    out_specs = P((X, C), RA)

    return jax.shard_map(body, mesh=torus, in_specs=in_specs, out_specs=out_specs, check_vma=False)
```

```python
import jax
import jax.numpy as jnp
from jax import lax
from jax.experimental import pallas as pl
from jax.experimental.pallas import tpu as pltpu
from jax.sharding import Mesh
from jax.sharding import PartitionSpec as P


Z, Y, X, C = "ra_0", "ra_1", "cb", "dp"
RA = (Z, Y)
ALL = (Z, Y, X, C)
RESID = 1.4142135
EPS = 0.5
BF = jnp.bfloat16
F32 = jnp.float32
NZ, NY = 8, 4


def place(z, y, core):
    z, y = (z - core) % NZ, (y - core) % NY
    return (y % 2) * 2 + z % 2, y // 2, z // 2


def label(zh, p, core):
    return (zh - core * (1 - p % 2)) % (NZ // 2)


def pairs_of(sizes):
    nz, ny, nx, nc = sizes
    near, far = {}, {}
    for z in range(nz):
        for y in range(ny):
            for x in range(nx):
                for c in range(nc):
                    at = ((z * ny + y) * nx + x) * nc + c
                    p, yh, zh = place(z, y, c)
                    near.setdefault((x, c, yh, zh), {})[p] = at
                    far.setdefault((x, c, p), {})[yh * (nz // 2) + label(zh, p, c)] = at

    def flips(groups, by):
        return [(g[i], g[i ^ by]) for g in groups.values() for i in g]

    return {
        "near": [flips(near, d) for d in range(4)],
        "mid": [flips(far, (e >> 1) * (nz // 2) + (e & 1)) for e in range(4)],
        "last": flips(far, 2),
    }


def stage(blocks, pairs):
    got = {d: lax.ppermute(blocks[d], ALL, pairs[d]) for d in (1, 2, 3)}
    own, diagonal, one, two = blocks[0], got[3], got[1], got[2]
    return [own, one, two, diagonal]


def gathered(pair, pairs):
    bundle = jnp.stack(stage([pair] * 4, pairs["mid"]))
    return stage([bundle] * 4, pairs["near"])


def scattered_sum(parts, pairs):
    some = sum(p.astype(F32) for p in stage(parts, pairs["near"])).astype(BF)
    return sum(p.astype(F32) for p in stage([some[e] for e in range(4)], pairs["mid"]))


def stats_to_all(row):
    n = lax.axis_size(RA)
    return lax.all_to_all(jnp.broadcast_to(row[None], (n, *row.shape)), RA, 0, 0, tiled=True)


def shift(a, axis, by):
    n = lax.axis_size(axis)
    return lax.ppermute(a, axis, [(i, (i + by) % n) for i in range(n)])


def half_of(w):
    rows = w.shape[0] // 2
    return lax.dynamic_slice_in_dim(w, lax.axis_index(C) * rows, rows, 0)


def packed(up, down):
    up, down = half_of(up), half_of(down)
    width = up.shape[1]
    return jnp.concatenate([up] + [down[:, i : i + width] for i in range(0, down.shape[1], width)], axis=0)


def split3(v):
    hi = lax.reduce_precision(v, 8, 7)
    mid = lax.reduce_precision(v - hi, 8, 7)
    return [hi, mid, v - hi - mid]


def from_peer(idx, d, e, g):
    core, p, yh, zh = idx[1], idx[2] ^ d, idx[3], idx[4]
    turn = core & (1 - (p & 1))
    zh = ((((zh - turn) & (NZ // 2 - 1)) ^ (g * 2 + (e & 1))) + turn) & (NZ // 2 - 1)
    z = (zh * 2 + (p & 1) + core) & (NZ - 1)
    y = ((yh ^ (e >> 1)) * 2 + (p >> 1) + core) & (NY - 1)
    return z * NY + y


def to_peer(idx, d, j, yh):
    core, p = idx[1], idx[2] ^ d
    turn = core & (1 - (p & 1))
    zz = (p & 1) ^ core
    zh = (j - core * (1 - zz)) & (NZ // 2 - 1)
    y = (yh * 2 + (p >> 1) + core) & (NY - 1)
    flip = ((zh - turn) & (NZ // 2 - 1)) ^ ((idx[4] - turn) & (NZ // 2 - 1))
    return (2 * j + zz) * NY + y, (flip & 1) + 2 * (yh ^ idx[3]), flip >> 1


def matmuls(idx, xs, up, down, pieces, hv, ov, outs):
    nx = 1 + len(pieces)
    me, core = idx[0], idx[1]
    per = xs.shape[0] // nx
    wide = hv.shape[2]

    def features(first, count):
        return jnp.concatenate([xs[first + k] for k in range(count)], axis=1)

    pre = jnp.dot(features(per * me, per), up[...], preferred_element_type=F32)
    for by, mine, other in pieces:
        source = lax.rem(me + (nx - by), nx)
        for half, piece in ((core, mine), (1 - core, other)):
            rows = features(per * source + per // 2 * half, per // 2)
            pre = pre + jnp.dot(rows, piece(0, per // 2 * 128), preferred_element_type=F32)
    hidden = jnp.square(jnp.maximum(pre, 0.0)).astype(BF)
    for half in range(2):
        hv[half] = hidden[:, half * wide : (half + 1) * wide]

    def emit(j, at, part):
        part = part.astype(BF)
        for i in range(part.shape[1] // 128):
            ov[per * j + at + i] = part[:, i * 128 : (i + 1) * 128]

    def send(j):
        for d in range(4):
            for yh in range(NY // 2):
                slot, e, g = to_peer(idx, d, j, yh)
                outs[d][e, g] = ov[slot]

    part = jnp.dot(hv[0], down[:wide], preferred_element_type=F32)
    emit(me, 0, part + jnp.dot(hv[1], down[wide:], preferred_element_type=F32))
    send(me)
    for by, mine, other in pieces:
        source = lax.rem(me + (nx - by), nx)
        for k in range(2):
            first = per // 2 * 128 + k * wide
            part = jnp.dot(hv[core], mine(first, wide), preferred_element_type=F32)
            part = part + jnp.dot(hv[1 - core], other(first, wide), preferred_element_type=F32)
            emit(source, k * per // 2, part)
        send(source)


def whole(ref):
    return lambda first, count: ref[first : first + count]


def split(top, low):
    cut = top.shape[0]
    return lambda first, count: top[first : first + count] if first < cut else low[first - cut : first - cut + count]


def first_kernel(
    idx, x0, x1, x2, x3, up, down, m1, m3, fu, fd, o1, o3, pu, pd, u0, u1, u2, u3, xs, hv, ov
):
    for d, x in enumerate((x0, x1, x2, x3)):
        for i in range(8):
            xs[from_peer(idx, d, i // 2, i % 2)] = x[i // 2, i % 2]
    pieces = [(1, whole(m1), whole(o1)), (3, whole(m3), whole(o3)), (2, split(fu, fd), split(pu, pd))]
    matmuls(idx, xs, up, down, pieces, hv, ov, (u0, u1, u2, u3))


def second_kernel(
    idx, x0, x1, x2, x3, up, down, m1, m2, m3, o1, o2, o3, mixed, own_gain, own_bias, u0, u1, u2, u3, own,
    xs, gain, bias, hv, ov,
):
    nb, tokens = xs.shape[:2]
    step = 64
    width = nb * 128
    blocks = []
    for d, x in enumerate((x0, x1, x2, x3)):
        for i in range(8):
            b = from_peer(idx, d, i // 2, i % 2)
            blocks.append((x, i // 2, i % 2, b))
            t = x[i // 2, i % 2, tokens : tokens + 8, :].astype(F32)
            gain[pl.ds(b, 1)] = t[0:1] + t[1:2] + t[2:3]
            bias[pl.ds(b, 1)] = t[3:4] + t[4:5] + t[5:6]

    def norm(i, carry):
        rows = pl.ds(pl.multiple_of(i * step, step), step)
        acc = jnp.zeros((step, 128), F32)
        squares = jnp.zeros((step, 128), F32)
        for x, e, g, b in blocks:
            v = x[e, g, rows, :].astype(F32)
            acc = acc + v
            squares = squares + v * v
        mean = jnp.sum(acc, axis=1, keepdims=True) / width
        var = jnp.sum(squares, axis=1, keepdims=True) / width - mean * mean
        scale = lax.rsqrt(jnp.maximum(var, 0.0) + EPS)
        for x, e, g, b in blocks:
            v = (x[e, g, rows, :].astype(F32) - mean) * scale
            xs[b, rows, :] = (v * gain[pl.ds(b, 1)] + bias[pl.ds(b, 1)]).astype(BF)
        own[rows, :] = ((mixed[rows, :] - mean) * scale * own_gain[...] + own_bias[...]).astype(BF)
        return carry

    lax.fori_loop(0, tokens // step, norm, 0)
    pieces = [(1, whole(m1), whole(o1)), (3, whole(m2), whole(o2)), (2, whole(m3), whole(o3))]
    matmuls(idx, xs, up, down, pieces, hv, ov, (u0, u1, u2, u3))


ANY = pl.BlockSpec(memory_space=pltpu.MemorySpace.HBM)
VMEM = pl.BlockSpec(memory_space=pltpu.MemorySpace.VMEM)
SMEM = pl.BlockSpec(memory_space=pltpu.MemorySpace.SMEM)


def ffn(kernel, idx, x, tokens, up, down, pieces, extra, own_out, norm_scratch):
    nx, nb = lax.axis_size(X), NZ * NY
    width, ff = up.shape[0] * nx, up.shape[1]
    near = [pltpu.with_memory_space_constraint(a, pltpu.MemorySpace.VMEM) for a in (*x, up, down, *pieces)]
    return pl.pallas_call(
        kernel,
        out_shape=[pltpu.VMEM((4, nb // 16, tokens, 128), BF)] * 4 + own_out,
        in_specs=[SMEM] + [VMEM] * (len(near) + len(extra)),
        out_specs=[VMEM] * (4 + len(own_out)),
        scratch_shapes=[pltpu.VMEM((nb, tokens, 128), BF)]
        + norm_scratch
        + [
            pltpu.VMEM((2, tokens, ff // 2), BF),
            pltpu.VMEM((nb, tokens, 128), BF),
        ],
        compiler_params=pltpu.CompilerParams(vmem_limit_bytes=28 << 20),
        cost_estimate=pl.CostEstimate(flops=4 * tokens * width * ff, bytes_accessed=14 << 20, transcendentals=0),
    )(idx, *near, *extra)


def body(
    stream,
    up_first,
    down_first,
    up_second,
    down_second,
    gain_first,
    bias_first,
    gain_second,
    bias_second,
):
    tokens = stream.shape[0]
    pairs = pairs_of([lax.axis_size(axis) for axis in ALL])
    pair = jnp.stack([stream, lax.ppermute(stream, ALL, pairs["last"])])
    w = packed(up_first, down_first)
    left, right = shift(w, X, 1), shift(w, X, -1)
    x_all = gathered(pair, pairs)
    cut = w.shape[0] // 2
    mine_1 = [left, right, shift(left[:cut], X, 1), shift(right[cut:], X, -1)]
    others_1 = [shift(m, C, 1) for m in mine_1]
    w = packed(up_second, down_second)
    mine_2 = [shift(w, X, by) for by in (1, -1, 2)]
    core = lax.axis_index(C)
    p, yh, zh = place(lax.axis_index(Z), lax.axis_index(Y), core)
    idx = jnp.stack([lax.axis_index(X), core, p, yh, zh]).astype(jnp.int32)
    parts = ffn(first_kernel, idx, x_all, tokens, up_first, down_first, mine_1 + others_1, [], [], [])
    tail = jnp.stack(split3(gain_first) + split3(bias_first) + [jnp.zeros_like(gain_first)] * 2).astype(BF)
    tails = jnp.broadcast_to(tail[None], (2, *tail.shape))
    some = jnp.concatenate([scattered_sum(parts, pairs).astype(BF), tails], axis=1)
    there = lax.ppermute(some, ALL, pairs["last"])[::-1]
    mixed = RESID * pair.astype(F32) + some[:, :tokens].astype(F32) + there[:, :tokens].astype(F32)
    tails = jnp.stack([tail, there[1, tokens:]])
    mixed_all = gathered(jnp.concatenate([mixed.astype(BF), tails], axis=1), pairs)
    others_2 = [shift(m, C, 1) for m in mine_2]
    nb = NZ * NY
    *parts, x = ffn(
        second_kernel, idx, mixed_all, tokens, up_second, down_second, mine_2 + others_2,
        [mixed[0], gain_first[None], bias_first[None]],
        [pltpu.VMEM((tokens, 128), BF)],
        [pltpu.VMEM((nb, 128), F32), pltpu.VMEM((nb, 128), F32)],
    )
    some = scattered_sum(parts, pairs)
    branch = some[0] + lax.ppermute(some[1].astype(BF), ALL, pairs["last"]).astype(F32)
    mixed = RESID * x.astype(F32) + branch
    width = mixed.shape[1] * lax.axis_size(RA)
    sums = jnp.concatenate([jnp.sum(mixed, axis=1), jnp.sum(mixed * mixed, axis=1)])
    sums = jnp.sum(stats_to_all(sums[None]), axis=0)[0]
    mean = sums[:tokens, None] / width
    var = sums[tokens:, None] / width - mean * mean
    return ((mixed - mean) * lax.rsqrt(var + EPS) * gain_second + bias_second).astype(BF)


def solution(mesh):
    torus = Mesh(mesh.devices.reshape(NZ, NY, mesh.shape["cb"], mesh.shape["dp"]), (Z, Y, X, C))
    in_specs = (
        P((X, C), RA),
        P(X, RA),
        P(RA, X),
        P(X, RA),
        P(RA, X),
        P(RA),
        P(RA),
        P(RA),
        P(RA),
    )
    out_specs = P((X, C), RA)

    return jax.shard_map(body, mesh=torus, in_specs=in_specs, out_specs=out_specs, check_vma=False)
```

```python
import jax
import jax.numpy as jnp
from jax import lax
from jax.experimental import pallas as pl
from jax.experimental.pallas import tpu as pltpu
from jax.sharding import Mesh
from jax.sharding import PartitionSpec as P


Z, Y, X, C = "ra_0", "ra_1", "cb", "dp"
RA = (Z, Y)
ALL = (Z, Y, X, C)
RESID = 1.4142135
EPS = 0.5
BF = jnp.bfloat16
F32 = jnp.float32
NZ, NY = 8, 4


def place(z, y, core):
    z, y = (z - core) % NZ, (y - core) % NY
    return (y % 2) * 2 + z % 2, y // 2, z // 2


def label(zh, p, core):
    return (zh - core * (1 - p % 2)) % (NZ // 2)


def pairs_of(sizes):
    nz, ny, nx, nc = sizes
    near, far = {}, {}
    for z in range(nz):
        for y in range(ny):
            for x in range(nx):
                for c in range(nc):
                    at = ((z * ny + y) * nx + x) * nc + c
                    p, yh, zh = place(z, y, c)
                    near.setdefault((x, c, yh, zh), {})[p] = at
                    far.setdefault((x, c, p), {})[yh * (nz // 2) + label(zh, p, c)] = at

    def flips(groups, by):
        return [(g[i], g[i ^ by]) for g in groups.values() for i in g]

    return {
        "near": [flips(near, d) for d in range(4)],
        "mid": [flips(far, (e >> 1) * (nz // 2) + (e & 1)) for e in range(4)],
        "last": flips(far, 2),
    }


def stage(blocks, pairs):
    got = {d: lax.ppermute(blocks[d], ALL, pairs[d]) for d in (1, 2, 3)}
    own, diagonal, one, two = blocks[0], got[3], got[1], got[2]
    return [own, one, two, diagonal]


def gathered(pair, pairs):
    bundle = jnp.stack(stage([pair] * 4, pairs["mid"]))
    return stage([bundle] * 4, pairs["near"])


def scattered_sum(parts, pairs):
    some = sum(p.astype(F32) for p in stage(parts, pairs["near"])).astype(BF)
    return sum(p.astype(F32) for p in stage([some[e] for e in range(4)], pairs["mid"]))


def stats_to_all(row):
    n = lax.axis_size(RA)
    return lax.all_to_all(jnp.broadcast_to(row[None], (n, *row.shape)), RA, 0, 0, tiled=True)


def shift(a, axis, by):
    n = lax.axis_size(axis)
    return lax.ppermute(a, axis, [(i, (i + by) % n) for i in range(n)])


def half_of(w):
    rows = w.shape[0] // 2
    return lax.dynamic_slice_in_dim(w, lax.axis_index(C) * rows, rows, 0)


def packed(up, down):
    up, down = half_of(up), half_of(down)
    width = up.shape[1]
    return jnp.concatenate([up] + [down[:, i : i + width] for i in range(0, down.shape[1], width)], axis=0)


def split3(v):
    hi = lax.reduce_precision(v, 8, 7)
    mid = lax.reduce_precision(v - hi, 8, 7)
    return [hi, mid, v - hi - mid]


def from_peer(idx, d, e, g):
    core, p, yh, zh = idx[1], idx[2] ^ d, idx[3], idx[4]
    turn = core & (1 - (p & 1))
    zh = ((((zh - turn) & (NZ // 2 - 1)) ^ (g * 2 + (e & 1))) + turn) & (NZ // 2 - 1)
    z = (zh * 2 + (p & 1) + core) & (NZ - 1)
    y = ((yh ^ (e >> 1)) * 2 + (p >> 1) + core) & (NY - 1)
    return z * NY + y


def to_peer(idx, d, j, yh):
    core, p = idx[1], idx[2] ^ d
    turn = core & (1 - (p & 1))
    zz = (p & 1) ^ core
    zh = (j - core * (1 - zz)) & (NZ // 2 - 1)
    y = (yh * 2 + (p >> 1) + core) & (NY - 1)
    flip = ((zh - turn) & (NZ // 2 - 1)) ^ ((idx[4] - turn) & (NZ // 2 - 1))
    return (2 * j + zz) * NY + y, (flip & 1) + 2 * (yh ^ idx[3]), flip >> 1


def matmuls(idx, xs, up, down, copies, pieces, hv, ov, outs):
    nx = 1 + len(pieces)
    me, core = idx[0], idx[1]
    per = xs.shape[0] // nx
    wide = hv.shape[2]

    def features(first, count):
        return jnp.concatenate([xs[first + k] for k in range(count)], axis=1)

    pre = None
    for by, mine, other in pieces:
        source = lax.rem(me + (nx - by), nx)
        for half, piece in ((core, mine), (1 - core, other)):
            rows = features(per * source + per // 2 * half, per // 2)
            term = jnp.dot(rows, piece(0, per // 2 * 128), preferred_element_type=F32)
            pre = term if pre is None else pre + term
    for copy in copies:
        copy.wait()
    pre = pre + jnp.dot(features(per * me, per), up[...], preferred_element_type=F32)
    hidden = jnp.square(jnp.maximum(pre, 0.0)).astype(BF)
    for half in range(2):
        hv[half] = hidden[:, half * wide : (half + 1) * wide]

    def emit(j, at, part):
        part = part.astype(BF)
        for i in range(part.shape[1] // 128):
            ov[per * j + at + i] = part[:, i * 128 : (i + 1) * 128]

    def send(j):
        for d in range(4):
            for yh in range(NY // 2):
                slot, e, g = to_peer(idx, d, j, yh)
                outs[d][e, g] = ov[slot]

    part = jnp.dot(hv[0], down[:wide], preferred_element_type=F32)
    emit(me, 0, part + jnp.dot(hv[1], down[wide:], preferred_element_type=F32))
    send(me)
    for by, mine, other in pieces:
        source = lax.rem(me + (nx - by), nx)
        for k in range(2):
            first = per // 2 * 128 + k * wide
            part = jnp.dot(hv[core], mine(first, wide), preferred_element_type=F32)
            part = part + jnp.dot(hv[1 - core], other(first, wide), preferred_element_type=F32)
            emit(source, k * per // 2, part)
        send(source)


def fetch(up, down, upv, dv, sems):
    copies = [pltpu.make_async_copy(up, upv, sems.at[0]), pltpu.make_async_copy(down, dv, sems.at[1])]
    for copy in copies:
        copy.start()
    return copies


def whole(ref):
    return lambda first, count: ref[first : first + count]


def split(top, low):
    cut = top.shape[0]
    return lambda first, count: top[first : first + count] if first < cut else low[first - cut : first - cut + count]


def first_kernel(
    idx, x0, x1, x2, x3, up, down, m1, m3, fu, fd, o1, o3, pu, pd, u0, u1, u2, u3, xs, hv, ov, upv, dv, sems
):
    copies = fetch(up, down, upv, dv, sems)
    for d, x in enumerate((x0, x1, x2, x3)):
        for i in range(8):
            xs[from_peer(idx, d, i // 2, i % 2)] = x[i // 2, i % 2]
    pieces = [(1, whole(m1), whole(o1)), (3, whole(m3), whole(o3)), (2, split(fu, fd), split(pu, pd))]
    matmuls(idx, xs, upv, dv, copies, pieces, hv, ov, (u0, u1, u2, u3))


def second_kernel(
    idx, x0, x1, x2, x3, up, down, m1, m2, m3, o1, o2, o3, mixed, own_gain, own_bias, u0, u1, u2, u3, own,
    xs, gain, bias, hv, ov, upv, dv, sems,
):
    copies = fetch(up, down, upv, dv, sems)
    nb, tokens = xs.shape[:2]
    step = 64
    width = nb * 128
    blocks = []
    for d, x in enumerate((x0, x1, x2, x3)):
        for i in range(8):
            b = from_peer(idx, d, i // 2, i % 2)
            blocks.append((x, i // 2, i % 2, b))
            t = x[i // 2, i % 2, tokens : tokens + 8, :].astype(F32)
            gain[pl.ds(b, 1)] = t[0:1] + t[1:2] + t[2:3]
            bias[pl.ds(b, 1)] = t[3:4] + t[4:5] + t[5:6]

    def norm(i, carry):
        rows = pl.ds(pl.multiple_of(i * step, step), step)
        acc = jnp.zeros((step, 128), F32)
        squares = jnp.zeros((step, 128), F32)
        for x, e, g, b in blocks:
            v = x[e, g, rows, :].astype(F32)
            acc = acc + v
            squares = squares + v * v
        mean = jnp.sum(acc, axis=1, keepdims=True) / width
        var = jnp.sum(squares, axis=1, keepdims=True) / width - mean * mean
        scale = lax.rsqrt(jnp.maximum(var, 0.0) + EPS)
        for x, e, g, b in blocks:
            v = (x[e, g, rows, :].astype(F32) - mean) * scale
            xs[b, rows, :] = (v * gain[pl.ds(b, 1)] + bias[pl.ds(b, 1)]).astype(BF)
        own[rows, :] = ((mixed[rows, :] - mean) * scale * own_gain[...] + own_bias[...]).astype(BF)
        return carry

    lax.fori_loop(0, tokens // step, norm, 0)
    pieces = [(1, whole(m1), whole(o1)), (3, whole(m2), whole(o2)), (2, whole(m3), whole(o3))]
    matmuls(idx, xs, upv, dv, copies, pieces, hv, ov, (u0, u1, u2, u3))


ANY = pl.BlockSpec(memory_space=pltpu.MemorySpace.HBM)
VMEM = pl.BlockSpec(memory_space=pltpu.MemorySpace.VMEM)
SMEM = pl.BlockSpec(memory_space=pltpu.MemorySpace.SMEM)


def ffn(kernel, idx, x, tokens, up, down, pieces, extra, own_out, norm_scratch):
    nx, nb = lax.axis_size(X), NZ * NY
    width, ff = up.shape[0] * nx, up.shape[1]
    near = [pltpu.with_memory_space_constraint(a, pltpu.MemorySpace.VMEM) for a in (*x, *pieces)]
    far = [pltpu.with_memory_space_constraint(a, pltpu.MemorySpace.HBM) for a in (up, down)]
    return pl.pallas_call(
        kernel,
        out_shape=[pltpu.VMEM((4, nb // 16, tokens, 128), BF)] * 4 + own_out,
        in_specs=[SMEM] + [VMEM] * 4 + [ANY] * 2 + [VMEM] * (len(pieces) + len(extra)),
        out_specs=[VMEM] * (4 + len(own_out)),
        scratch_shapes=[pltpu.VMEM((nb, tokens, 128), BF)]
        + norm_scratch
        + [
            pltpu.VMEM((2, tokens, ff // 2), BF),
            pltpu.VMEM((nb, tokens, 128), BF),
            pltpu.VMEM(up.shape, BF),
            pltpu.VMEM(down.shape, BF),
            pltpu.SemaphoreType.DMA((2,)),
        ],
        compiler_params=pltpu.CompilerParams(vmem_limit_bytes=28 << 20),
        cost_estimate=pl.CostEstimate(flops=4 * tokens * width * ff, bytes_accessed=14 << 20, transcendentals=0),
    )(idx, *near[:4], *far, *near[4:], *extra)


def body(
    stream,
    up_first,
    down_first,
    up_second,
    down_second,
    gain_first,
    bias_first,
    gain_second,
    bias_second,
):
    tokens = stream.shape[0]
    pairs = pairs_of([lax.axis_size(axis) for axis in ALL])
    pair = jnp.stack([stream, lax.ppermute(stream, ALL, pairs["last"])])
    w = packed(up_first, down_first)
    left, right = shift(w, X, 1), shift(w, X, -1)
    x_all = gathered(pair, pairs)
    cut = w.shape[0] // 2
    mine_1 = [left, right, shift(left[:cut], X, 1), shift(right[cut:], X, -1)]
    others_1 = [shift(m, C, 1) for m in mine_1]
    w = packed(up_second, down_second)
    mine_2 = [shift(w, X, by) for by in (1, -1, 2)]
    core = lax.axis_index(C)
    p, yh, zh = place(lax.axis_index(Z), lax.axis_index(Y), core)
    idx = jnp.stack([lax.axis_index(X), core, p, yh, zh]).astype(jnp.int32)
    parts = ffn(first_kernel, idx, x_all, tokens, up_first, down_first, mine_1 + others_1, [], [], [])
    tail = jnp.stack(split3(gain_first) + split3(bias_first) + [jnp.zeros_like(gain_first)] * 2).astype(BF)
    tails = jnp.broadcast_to(tail[None], (2, *tail.shape))
    some = jnp.concatenate([scattered_sum(parts, pairs).astype(BF), tails], axis=1)
    there = lax.ppermute(some, ALL, pairs["last"])[::-1]
    mixed = RESID * pair.astype(F32) + some[:, :tokens].astype(F32) + there[:, :tokens].astype(F32)
    tails = jnp.stack([tail, there[1, tokens:]])
    mixed_all = gathered(jnp.concatenate([mixed.astype(BF), tails], axis=1), pairs)
    others_2 = [shift(m, C, 1) for m in mine_2]
    nb = NZ * NY
    *parts, x = ffn(
        second_kernel, idx, mixed_all, tokens, up_second, down_second, mine_2 + others_2,
        [mixed[0], gain_first[None], bias_first[None]],
        [pltpu.VMEM((tokens, 128), BF)],
        [pltpu.VMEM((nb, 128), F32), pltpu.VMEM((nb, 128), F32)],
    )
    some = scattered_sum(parts, pairs)
    branch = some[0] + lax.ppermute(some[1].astype(BF), ALL, pairs["last"]).astype(F32)
    mixed = RESID * x.astype(F32) + branch
    width = mixed.shape[1] * lax.axis_size(RA)
    sums = jnp.concatenate([jnp.sum(mixed, axis=1), jnp.sum(mixed * mixed, axis=1)])
    sums = jnp.sum(stats_to_all(sums[None]), axis=0)[0]
    mean = sums[:tokens, None] / width
    var = sums[tokens:, None] / width - mean * mean
    return ((mixed - mean) * lax.rsqrt(var + EPS) * gain_second + bias_second).astype(BF)


def solution(mesh):
    torus = Mesh(mesh.devices.reshape(NZ, NY, mesh.shape["cb"], mesh.shape["dp"]), (Z, Y, X, C))
    in_specs = (
        P((X, C), RA),
        P(X, RA),
        P(RA, X),
        P(X, RA),
        P(RA, X),
        P(RA),
        P(RA),
        P(RA),
        P(RA),
    )
    out_specs = P((X, C), RA)

    return jax.shard_map(body, mesh=torus, in_specs=in_specs, out_specs=out_specs, check_vma=False)
```

```python
import jax
import jax.numpy as jnp
from jax import lax
from jax.experimental import pallas as pl
from jax.experimental.pallas import tpu as pltpu
from jax.sharding import Mesh
from jax.sharding import PartitionSpec as P


Z, Y, X, C = "ra_0", "ra_1", "cb", "dp"
RA = (Z, Y)
ALL = (Z, Y, X, C)
RESID = 1.4142135
EPS = 0.5
BF = jnp.bfloat16
F32 = jnp.float32
NZ, NY = 8, 4


def place(z, y, core):
    z, y = (z - core) % NZ, (y - core) % NY
    return (y % 2) * 2 + z % 2, y // 2, z // 2


def label(zh, p, core):
    return (zh - core * (1 - p % 2)) % (NZ // 2)


def pairs_of(sizes):
    nz, ny, nx, nc = sizes
    near, far = {}, {}
    for z in range(nz):
        for y in range(ny):
            for x in range(nx):
                for c in range(nc):
                    at = ((z * ny + y) * nx + x) * nc + c
                    p, yh, zh = place(z, y, c)
                    near.setdefault((x, c, yh, zh), {})[p] = at
                    far.setdefault((x, c, p), {})[yh * (nz // 2) + label(zh, p, c)] = at

    def flips(groups, by):
        return [(g[i], g[i ^ by]) for g in groups.values() for i in g]

    return {
        "near": [flips(near, d) for d in range(4)],
        "mid": [flips(far, (e >> 1) * (nz // 2) + (e & 1)) for e in range(4)],
        "last": flips(far, 2),
    }


def stage(blocks, pairs):
    got = {d: lax.ppermute(blocks[d], ALL, pairs[d]) for d in (1, 2, 3)}
    own, diagonal, one, two = blocks[0], got[3], got[1], got[2]
    return [own, one, two, diagonal]


def gathered(pair, pairs):
    bundle = jnp.stack(stage([pair] * 4, pairs["mid"]))
    return stage([bundle] * 4, pairs["near"])


def scattered_sum(parts, pairs):
    def near_sum(some):
        return sum(p.astype(F32) for p in stage(some, pairs["near"])).astype(BF)

    def flip(block, e):
        return lax.ppermute(block, ALL, pairs["mid"][e]).astype(F32)

    high = near_sum(parts[4:])
    low = near_sum(parts[:4])
    far = flip(high[0], 2) + flip(high[1], 3)
    return low[0].astype(F32) + flip(low[1], 1) + far


def stats_to_all(row):
    n = lax.axis_size(RA)
    return lax.all_to_all(jnp.broadcast_to(row[None], (n, *row.shape)), RA, 0, 0, tiled=True)


def shift(a, axis, by):
    n = lax.axis_size(axis)
    return lax.ppermute(a, axis, [(i, (i + by) % n) for i in range(n)])


def half_of(w):
    rows = w.shape[0] // 2
    return lax.dynamic_slice_in_dim(w, lax.axis_index(C) * rows, rows, 0)


def packed(up, down):
    up, down = half_of(up), half_of(down)
    width = up.shape[1]
    return jnp.concatenate([up] + [down[:, i : i + width] for i in range(0, down.shape[1], width)], axis=0)


def split3(v):
    hi = lax.reduce_precision(v, 8, 7)
    mid = lax.reduce_precision(v - hi, 8, 7)
    return [hi, mid, v - hi - mid]


def from_peer(idx, d, e, g):
    core, p, yh, zh = idx[1], idx[2] ^ d, idx[3], idx[4]
    turn = core & (1 - (p & 1))
    zh = ((((zh - turn) & (NZ // 2 - 1)) ^ (g * 2 + (e & 1))) + turn) & (NZ // 2 - 1)
    z = (zh * 2 + (p & 1) + core) & (NZ - 1)
    y = ((yh ^ (e >> 1)) * 2 + (p >> 1) + core) & (NY - 1)
    return z * NY + y


def to_peer(idx, d, j, yh):
    core, p = idx[1], idx[2] ^ d
    turn = core & (1 - (p & 1))
    zz = (p & 1) ^ core
    zh = (j - core * (1 - zz)) & (NZ // 2 - 1)
    y = (yh * 2 + (p >> 1) + core) & (NY - 1)
    flip = ((zh - turn) & (NZ // 2 - 1)) ^ ((idx[4] - turn) & (NZ // 2 - 1))
    return (2 * j + zz) * NY + y, (flip & 1) + 2 * (yh ^ idx[3]), flip >> 1


def matmuls(idx, xs, up, down, copies, pieces, hv, ov, outs):
    nx = 1 + len(pieces)
    me, core = idx[0], idx[1]
    per = xs.shape[0] // nx
    wide = hv.shape[2]

    def features(first, count):
        return jnp.concatenate([xs[first + k] for k in range(count)], axis=1)

    pre = None
    for by, mine, other in pieces:
        source = lax.rem(me + (nx - by), nx)
        for half, piece in ((core, mine), (1 - core, other)):
            rows = features(per * source + per // 2 * half, per // 2)
            term = jnp.dot(rows, piece(0, per // 2 * 128), preferred_element_type=F32)
            pre = term if pre is None else pre + term
    for copy in copies:
        copy.wait()
    pre = pre + jnp.dot(features(per * me, per), up[...], preferred_element_type=F32)
    hidden = jnp.square(jnp.maximum(pre, 0.0)).astype(BF)
    for half in range(2):
        hv[half] = hidden[:, half * wide : (half + 1) * wide]

    def emit(j, at, part):
        part = part.astype(BF)
        for i in range(part.shape[1] // 128):
            ov[per * j + at + i] = part[:, i * 128 : (i + 1) * 128]

    def send(j):
        for d in range(4):
            for f in range(2):
                slot, e, g = to_peer(idx, d, j, idx[3] ^ f)
                outs[4 * f + d][e & 1, g] = ov[slot]

    part = jnp.dot(hv[0], down[:wide], preferred_element_type=F32)
    emit(me, 0, part + jnp.dot(hv[1], down[wide:], preferred_element_type=F32))
    send(me)
    for by, mine, other in pieces:
        source = lax.rem(me + (nx - by), nx)
        for k in range(2):
            first = per // 2 * 128 + k * wide
            part = jnp.dot(hv[core], mine(first, wide), preferred_element_type=F32)
            part = part + jnp.dot(hv[1 - core], other(first, wide), preferred_element_type=F32)
            emit(source, k * per // 2, part)
        send(source)


def fetch(up, down, upv, dv, sems):
    copies = [pltpu.make_async_copy(up, upv, sems.at[0]), pltpu.make_async_copy(down, dv, sems.at[1])]
    for copy in copies:
        copy.start()
    return copies


def whole(ref):
    return lambda first, count: ref[first : first + count]


def split(top, low):
    cut = top.shape[0]
    return lambda first, count: top[first : first + count] if first < cut else low[first - cut : first - cut + count]


def first_kernel(
    idx, x0, x1, x2, x3, up, down, m1, m3, fu, fd, o1, o3, pu, pd, u0, u1, u2, u3, v0, v1, v2, v3, xs, hv, ov, upv, dv, sems
):
    copies = fetch(up, down, upv, dv, sems)
    for d, x in enumerate((x0, x1, x2, x3)):
        for i in range(8):
            xs[from_peer(idx, d, i // 2, i % 2)] = x[i // 2, i % 2]
    pieces = [(1, whole(m1), whole(o1)), (3, whole(m3), whole(o3)), (2, split(fu, fd), split(pu, pd))]
    matmuls(idx, xs, upv, dv, copies, pieces, hv, ov, (u0, u1, u2, u3, v0, v1, v2, v3))


def second_kernel(
    idx, x0, x1, x2, x3, up, down, m1, m2, m3, others, mixed, own_gain, own_bias, u0, u1, u2, u3, v0, v1, v2, v3, own,
    xs, gain, bias, hv, ov, upv, dv, sems,
):
    copies = fetch(up, down, upv, dv, sems)
    nb, tokens = xs.shape[:2]
    step = 64
    width = nb * 128
    blocks = []
    for d, x in enumerate((x0, x1, x2, x3)):
        for i in range(8):
            b = from_peer(idx, d, i // 2, i % 2)
            blocks.append((x, i // 2, i % 2, b))
            t = x[i // 2, i % 2, tokens : tokens + 8, :].astype(F32)
            gain[pl.ds(b, 1)] = t[0:1] + t[1:2] + t[2:3]
            bias[pl.ds(b, 1)] = t[3:4] + t[4:5] + t[5:6]

    def norm(i, carry):
        rows = pl.ds(pl.multiple_of(i * step, step), step)
        acc = jnp.zeros((step, 128), F32)
        squares = jnp.zeros((step, 128), F32)
        for x, e, g, b in blocks:
            v = x[e, g, rows, :].astype(F32)
            acc = acc + v
            squares = squares + v * v
        mean = jnp.sum(acc, axis=1, keepdims=True) / width
        var = jnp.sum(squares, axis=1, keepdims=True) / width - mean * mean
        scale = lax.rsqrt(jnp.maximum(var, 0.0) + EPS)
        for x, e, g, b in blocks:
            v = (x[e, g, rows, :].astype(F32) - mean) * scale
            xs[b, rows, :] = (v * gain[pl.ds(b, 1)] + bias[pl.ds(b, 1)]).astype(BF)
        own[rows, :] = ((mixed[rows, :] - mean) * scale * own_gain[...] + own_bias[...]).astype(BF)
        return carry

    lax.fori_loop(0, tokens // step, norm, 0)
    pieces = [(by, whole(m), whole(others.at[k])) for k, (by, m) in enumerate(((1, m1), (3, m2), (2, m3)))]
    matmuls(idx, xs, upv, dv, copies, pieces, hv, ov, (u0, u1, u2, u3, v0, v1, v2, v3))


ANY = pl.BlockSpec(memory_space=pltpu.MemorySpace.HBM)
VMEM = pl.BlockSpec(memory_space=pltpu.MemorySpace.VMEM)
SMEM = pl.BlockSpec(memory_space=pltpu.MemorySpace.SMEM)


def ffn(kernel, idx, x, tokens, up, down, pieces, extra, own_out, norm_scratch):
    nx, nb = lax.axis_size(X), NZ * NY
    width, ff = up.shape[0] * nx, up.shape[1]
    near = [pltpu.with_memory_space_constraint(a, pltpu.MemorySpace.VMEM) for a in (*x, *pieces)]
    far = [pltpu.with_memory_space_constraint(a, pltpu.MemorySpace.HBM) for a in (up, down)]
    return pl.pallas_call(
        kernel,
        out_shape=[pltpu.VMEM((2, nb // 16, tokens, 128), BF)] * 8 + own_out,
        in_specs=[SMEM] + [VMEM] * 4 + [ANY] * 2 + [VMEM] * (len(pieces) + len(extra)),
        out_specs=[VMEM] * (8 + len(own_out)),
        scratch_shapes=[pltpu.VMEM((nb, tokens, 128), BF)]
        + norm_scratch
        + [
            pltpu.VMEM((2, tokens, ff // 2), BF),
            pltpu.VMEM((nb, tokens, 128), BF),
            pltpu.VMEM(up.shape, BF),
            pltpu.VMEM(down.shape, BF),
            pltpu.SemaphoreType.DMA((2,)),
        ],
        compiler_params=pltpu.CompilerParams(vmem_limit_bytes=28 << 20),
        cost_estimate=pl.CostEstimate(flops=4 * tokens * width * ff, bytes_accessed=14 << 20, transcendentals=0),
    )(idx, *near[:4], *far, *near[4:], *extra)


def body(
    stream,
    up_first,
    down_first,
    up_second,
    down_second,
    gain_first,
    bias_first,
    gain_second,
    bias_second,
):
    tokens = stream.shape[0]
    pairs = pairs_of([lax.axis_size(axis) for axis in ALL])
    pair = jnp.stack([stream, lax.ppermute(stream, ALL, pairs["last"])])
    w = packed(up_first, down_first)
    left, right = shift(w, X, 1), shift(w, X, -1)
    x_all = gathered(pair, pairs)
    cut = w.shape[0] // 2
    mine_1 = [left, right, shift(left[:cut], X, 1), shift(right[cut:], X, -1)]
    others_1 = [shift(m, C, 1) for m in mine_1]
    w = packed(up_second, down_second)
    mine_2 = [shift(w, X, by) for by in (1, -1, 2)]
    core = lax.axis_index(C)
    p, yh, zh = place(lax.axis_index(Z), lax.axis_index(Y), core)
    idx = jnp.stack([lax.axis_index(X), core, p, yh, zh]).astype(jnp.int32)
    parts = ffn(first_kernel, idx, x_all, tokens, up_first, down_first, mine_1 + others_1, [], [], [])
    tail = jnp.stack(split3(gain_first) + split3(bias_first) + [jnp.zeros_like(gain_first)] * 2).astype(BF)
    tails = jnp.broadcast_to(tail[None], (2, *tail.shape))
    some = jnp.concatenate([scattered_sum(parts, pairs).astype(BF), tails], axis=1)
    there = lax.ppermute(some, ALL, pairs["last"])[::-1]
    mixed = RESID * pair.astype(F32) + some[:, :tokens].astype(F32) + there[:, :tokens].astype(F32)
    tails = jnp.stack([tail, there[1, tokens:]])
    mixed_all = gathered(jnp.concatenate([mixed.astype(BF), tails], axis=1), pairs)
    others_2 = [shift(jnp.stack(mine_2), C, 1)]
    nb = NZ * NY
    *parts, x = ffn(
        second_kernel, idx, mixed_all, tokens, up_second, down_second, mine_2 + others_2,
        [mixed[0], gain_first[None], bias_first[None]],
        [pltpu.VMEM((tokens, 128), BF)],
        [pltpu.VMEM((nb, 128), F32), pltpu.VMEM((nb, 128), F32)],
    )
    some = scattered_sum(parts, pairs)
    branch = some[0] + lax.ppermute(some[1].astype(BF), ALL, pairs["last"]).astype(F32)
    mixed = RESID * x.astype(F32) + branch
    width = mixed.shape[1] * lax.axis_size(RA)
    sums = jnp.concatenate([jnp.sum(mixed, axis=1), jnp.sum(mixed * mixed, axis=1)])
    sums = jnp.sum(stats_to_all(sums[None]), axis=0)[0]
    mean = sums[:tokens, None] / width
    var = sums[tokens:, None] / width - mean * mean
    return ((mixed - mean) * lax.rsqrt(var + EPS) * gain_second + bias_second).astype(BF)


def solution(mesh):
    torus = Mesh(mesh.devices.reshape(NZ, NY, mesh.shape["cb"], mesh.shape["dp"]), (Z, Y, X, C))
    in_specs = (
        P((X, C), RA),
        P(X, RA),
        P(RA, X),
        P(X, RA),
        P(RA, X),
        P(RA),
        P(RA),
        P(RA),
        P(RA),
    )
    out_specs = P((X, C), RA)

    return jax.shard_map(body, mesh=torus, in_specs=in_specs, out_specs=out_specs, check_vma=False)
```

```python
import jax
import jax.numpy as jnp
from jax import lax
from jax.experimental import pallas as pl
from jax.experimental.pallas import tpu as pltpu
from jax.sharding import Mesh
from jax.sharding import PartitionSpec as P


Z, Y, X, C = "ra_0", "ra_1", "cb", "dp"
RA = (Z, Y)
ALL = (Z, Y, X, C)
RESID = 1.4142135
EPS = 0.5
BF = jnp.bfloat16
F32 = jnp.float32
NZ, NY = 8, 4


def place(z, y, core):
    z, y = (z - core) % NZ, (y - core) % NY
    return (y % 2) * 2 + z % 2, y // 2, z // 2


def label(zh, p, core):
    return (zh - core * (1 - p % 2)) % (NZ // 2)


def pairs_of(sizes):
    nz, ny, nx, nc = sizes
    near, far = {}, {}
    for z in range(nz):
        for y in range(ny):
            for x in range(nx):
                for c in range(nc):
                    at = ((z * ny + y) * nx + x) * nc + c
                    p, yh, zh = place(z, y, c)
                    near.setdefault((x, c, yh, zh), {})[p] = at
                    far.setdefault((x, c, p), {})[yh * (nz // 2) + label(zh, p, c)] = at

    def flips(groups, by):
        return [(g[i], g[i ^ by]) for g in groups.values() for i in g]

    return {
        "near": [flips(near, d) for d in range(4)],
        "mid": [flips(far, (e >> 1) * (nz // 2) + (e & 1)) for e in range(4)],
        "last": flips(far, 2),
    }


def stage(blocks, pairs):
    got = {d: lax.ppermute(blocks[d], ALL, pairs[d]) for d in (1, 2, 3)}
    own, diagonal, one, two = blocks[0], got[3], got[1], got[2]
    return [own, one, two, diagonal]


def gathered(pair, pairs):
    bundle = jnp.stack(stage([pair] * 4, pairs["mid"]))
    return stage([bundle] * 4, pairs["near"])


def scattered_sum(parts, pairs):
    def near_sum(some):
        return sum(p.astype(F32) for p in stage(some, pairs["near"])).astype(BF)

    def flip(block, e):
        return lax.ppermute(block, ALL, pairs["mid"][e]).astype(F32)

    if len(parts) == 4:
        some = near_sum(parts)
        return sum(p.astype(F32) for p in stage([some[e] for e in range(4)], pairs["mid"]))
    high = near_sum(parts[4:])
    low = near_sum(parts[:4])
    far = flip(high[0], 2) + flip(high[1], 3)
    return low[0].astype(F32) + flip(low[1], 1) + far


def stats_to_all(row):
    n = lax.axis_size(RA)
    return lax.all_to_all(jnp.broadcast_to(row[None], (n, *row.shape)), RA, 0, 0, tiled=True)


def shift(a, axis, by):
    n = lax.axis_size(axis)
    return lax.ppermute(a, axis, [(i, (i + by) % n) for i in range(n)])


def half_of(w):
    rows = w.shape[0] // 2
    return lax.dynamic_slice_in_dim(w, lax.axis_index(C) * rows, rows, 0)


def packed(up, down):
    up, down = half_of(up), half_of(down)
    width = up.shape[1]
    return jnp.concatenate([up] + [down[:, i : i + width] for i in range(0, down.shape[1], width)], axis=0)


def split3(v):
    hi = lax.reduce_precision(v, 8, 7)
    mid = lax.reduce_precision(v - hi, 8, 7)
    return [hi, mid, v - hi - mid]


def from_peer(idx, d, e, g):
    core, p, yh, zh = idx[1], idx[2] ^ d, idx[3], idx[4]
    turn = core & (1 - (p & 1))
    zh = ((((zh - turn) & (NZ // 2 - 1)) ^ (g * 2 + (e & 1))) + turn) & (NZ // 2 - 1)
    z = (zh * 2 + (p & 1) + core) & (NZ - 1)
    y = ((yh ^ (e >> 1)) * 2 + (p >> 1) + core) & (NY - 1)
    return z * NY + y


def to_peer(idx, d, j, yh):
    core, p = idx[1], idx[2] ^ d
    turn = core & (1 - (p & 1))
    zz = (p & 1) ^ core
    zh = (j - core * (1 - zz)) & (NZ // 2 - 1)
    y = (yh * 2 + (p >> 1) + core) & (NY - 1)
    flip = ((zh - turn) & (NZ // 2 - 1)) ^ ((idx[4] - turn) & (NZ // 2 - 1))
    return (2 * j + zz) * NY + y, (flip & 1) + 2 * (yh ^ idx[3]), flip >> 1


def matmuls(idx, xs, up, down, copies, pieces, hv, ov, outs):
    nx = 1 + len(pieces)
    me, core = idx[0], idx[1]
    per = xs.shape[0] // nx
    wide = hv.shape[2]

    def features(first, count):
        return jnp.concatenate([xs[first + k] for k in range(count)], axis=1)

    pre = None
    for by, mine, other in pieces:
        source = lax.rem(me + (nx - by), nx)
        for half, piece in ((core, mine), (1 - core, other)):
            rows = features(per * source + per // 2 * half, per // 2)
            term = jnp.dot(rows, piece(0, per // 2 * 128), preferred_element_type=F32)
            pre = term if pre is None else pre + term
    for copy in copies:
        copy.wait()
    pre = pre + jnp.dot(features(per * me, per), up[...], preferred_element_type=F32)
    hidden = jnp.square(jnp.maximum(pre, 0.0)).astype(BF)
    for half in range(2):
        hv[half] = hidden[:, half * wide : (half + 1) * wide]

    def emit(j, at, part):
        part = part.astype(BF)
        for i in range(part.shape[1] // 128):
            ov[per * j + at + i] = part[:, i * 128 : (i + 1) * 128]

    def send(j):
        for d in range(4):
            for f in range(2):
                slot, e, g = to_peer(idx, d, j, idx[3] ^ f)
                if len(outs) == 4:
                    outs[d][e, g] = ov[slot]
                else:
                    outs[4 * f + d][e & 1, g] = ov[slot]

    part = jnp.dot(hv[0], down[:wide], preferred_element_type=F32)
    emit(me, 0, part + jnp.dot(hv[1], down[wide:], preferred_element_type=F32))
    send(me)
    for by, mine, other in pieces:
        source = lax.rem(me + (nx - by), nx)
        for k in range(2):
            first = per // 2 * 128 + k * wide
            part = jnp.dot(hv[core], mine(first, wide), preferred_element_type=F32)
            part = part + jnp.dot(hv[1 - core], other(first, wide), preferred_element_type=F32)
            emit(source, k * per // 2, part)
        send(source)


def fetch(up, down, upv, dv, sems):
    copies = [pltpu.make_async_copy(up, upv, sems.at[0]), pltpu.make_async_copy(down, dv, sems.at[1])]
    for copy in copies:
        copy.start()
    return copies


def whole(ref):
    return lambda first, count: ref[first : first + count]


def split(top, low):
    cut = top.shape[0]
    return lambda first, count: top[first : first + count] if first < cut else low[first - cut : first - cut + count]


def first_kernel(
    idx, x0, x1, x2, x3, up, down, m1, m3, fu, fd, o1, o3, pu, pd, u0, u1, u2, u3, xs, hv, ov, upv, dv, sems
):
    copies = fetch(up, down, upv, dv, sems)
    for d, x in enumerate((x0, x1, x2, x3)):
        for i in range(8):
            xs[from_peer(idx, d, i // 2, i % 2)] = x[i // 2, i % 2]
    pieces = [(1, whole(m1), whole(o1)), (3, whole(m3), whole(o3)), (2, split(fu, fd), split(pu, pd))]
    matmuls(idx, xs, upv, dv, copies, pieces, hv, ov, (u0, u1, u2, u3))


def second_kernel(
    idx, x0, x1, x2, x3, up, down, m1, m2, m3, others, mixed, own_gain, own_bias, u0, u1, u2, u3, v0, v1, v2, v3, own,
    xs, gain, bias, hv, ov, upv, dv, sems,
):
    copies = fetch(up, down, upv, dv, sems)
    nb, tokens = xs.shape[:2]
    step = 64
    width = nb * 128
    blocks = []
    for d, x in enumerate((x0, x1, x2, x3)):
        for i in range(8):
            b = from_peer(idx, d, i // 2, i % 2)
            blocks.append((x, i // 2, i % 2, b))
            t = x[i // 2, i % 2, tokens : tokens + 8, :].astype(F32)
            gain[pl.ds(b, 1)] = t[0:1] + t[1:2] + t[2:3]
            bias[pl.ds(b, 1)] = t[3:4] + t[4:5] + t[5:6]

    def norm(i, carry):
        rows = pl.ds(pl.multiple_of(i * step, step), step)
        acc = jnp.zeros((step, 128), F32)
        squares = jnp.zeros((step, 128), F32)
        for x, e, g, b in blocks:
            v = x[e, g, rows, :].astype(F32)
            acc = acc + v
            squares = squares + v * v
        mean = jnp.sum(acc, axis=1, keepdims=True) / width
        var = jnp.sum(squares, axis=1, keepdims=True) / width - mean * mean
        scale = lax.rsqrt(jnp.maximum(var, 0.0) + EPS)
        for x, e, g, b in blocks:
            v = (x[e, g, rows, :].astype(F32) - mean) * scale
            xs[b, rows, :] = (v * gain[pl.ds(b, 1)] + bias[pl.ds(b, 1)]).astype(BF)
        own[rows, :] = ((mixed[rows, :] - mean) * scale * own_gain[...] + own_bias[...]).astype(BF)
        return carry

    lax.fori_loop(0, tokens // step, norm, 0)
    pieces = [(by, whole(m), whole(others.at[k])) for k, (by, m) in enumerate(((1, m1), (3, m2), (2, m3)))]
    matmuls(idx, xs, upv, dv, copies, pieces, hv, ov, (u0, u1, u2, u3, v0, v1, v2, v3))


ANY = pl.BlockSpec(memory_space=pltpu.MemorySpace.HBM)
VMEM = pl.BlockSpec(memory_space=pltpu.MemorySpace.VMEM)
SMEM = pl.BlockSpec(memory_space=pltpu.MemorySpace.SMEM)


def ffn(kernel, idx, x, tokens, up, down, pieces, extra, own_out, norm_scratch):
    nx, nb, cuts = lax.axis_size(X), NZ * NY, 1 + len(own_out)
    width, ff = up.shape[0] * nx, up.shape[1]
    near = [pltpu.with_memory_space_constraint(a, pltpu.MemorySpace.VMEM) for a in (*x, *pieces)]
    far = [pltpu.with_memory_space_constraint(a, pltpu.MemorySpace.HBM) for a in (up, down)]
    return pl.pallas_call(
        kernel,
        out_shape=[pltpu.VMEM((4 // cuts, nb // 16, tokens, 128), BF)] * (4 * cuts) + own_out,
        in_specs=[SMEM] + [VMEM] * 4 + [ANY] * 2 + [VMEM] * (len(pieces) + len(extra)),
        out_specs=[VMEM] * (4 * cuts + len(own_out)),
        scratch_shapes=[pltpu.VMEM((nb, tokens, 128), BF)]
        + norm_scratch
        + [
            pltpu.VMEM((2, tokens, ff // 2), BF),
            pltpu.VMEM((nb, tokens, 128), BF),
            pltpu.VMEM(up.shape, BF),
            pltpu.VMEM(down.shape, BF),
            pltpu.SemaphoreType.DMA((2,)),
        ],
        compiler_params=pltpu.CompilerParams(vmem_limit_bytes=28 << 20),
        cost_estimate=pl.CostEstimate(flops=4 * tokens * width * ff, bytes_accessed=14 << 20, transcendentals=0),
    )(idx, *near[:4], *far, *near[4:], *extra)


def body(
    stream,
    up_first,
    down_first,
    up_second,
    down_second,
    gain_first,
    bias_first,
    gain_second,
    bias_second,
):
    tokens = stream.shape[0]
    pairs = pairs_of([lax.axis_size(axis) for axis in ALL])
    pair = jnp.stack([stream, lax.ppermute(stream, ALL, pairs["last"])])
    w = packed(up_first, down_first)
    left, right = shift(w, X, 1), shift(w, X, -1)
    x_all = gathered(pair, pairs)
    cut = w.shape[0] // 2
    mine_1 = [left, right, shift(left[:cut], X, 1), shift(right[cut:], X, -1)]
    others_1 = [shift(m, C, 1) for m in mine_1]
    w = packed(up_second, down_second)
    mine_2 = [shift(w, X, by) for by in (1, -1, 2)]
    core = lax.axis_index(C)
    p, yh, zh = place(lax.axis_index(Z), lax.axis_index(Y), core)
    idx = jnp.stack([lax.axis_index(X), core, p, yh, zh]).astype(jnp.int32)
    parts = ffn(first_kernel, idx, x_all, tokens, up_first, down_first, mine_1 + others_1, [], [], [])
    tail = jnp.stack(split3(gain_first) + split3(bias_first) + [jnp.zeros_like(gain_first)] * 2).astype(BF)
    tails = jnp.broadcast_to(tail[None], (2, *tail.shape))
    some = jnp.concatenate([scattered_sum(parts, pairs).astype(BF), tails], axis=1)
    there = lax.ppermute(some, ALL, pairs["last"])[::-1]
    mixed = RESID * pair.astype(F32) + some[:, :tokens].astype(F32) + there[:, :tokens].astype(F32)
    tails = jnp.stack([tail, there[1, tokens:]])
    mixed_all = gathered(jnp.concatenate([mixed.astype(BF), tails], axis=1), pairs)
    others_2 = [shift(jnp.stack(mine_2), C, 1)]
    nb = NZ * NY
    *parts, x = ffn(
        second_kernel, idx, mixed_all, tokens, up_second, down_second, mine_2 + others_2,
        [mixed[0], gain_first[None], bias_first[None]],
        [pltpu.VMEM((tokens, 128), BF)],
        [pltpu.VMEM((nb, 128), F32), pltpu.VMEM((nb, 128), F32)],
    )
    some = scattered_sum(parts, pairs)
    branch = some[0] + lax.ppermute(some[1].astype(BF), ALL, pairs["last"]).astype(F32)
    mixed = RESID * x.astype(F32) + branch
    width = mixed.shape[1] * lax.axis_size(RA)
    sums = jnp.concatenate([jnp.sum(mixed, axis=1), jnp.sum(mixed * mixed, axis=1)])
    sums = jnp.sum(stats_to_all(sums[None]), axis=0)[0]
    mean = sums[:tokens, None] / width
    var = sums[tokens:, None] / width - mean * mean
    return ((mixed - mean) * lax.rsqrt(var + EPS) * gain_second + bias_second).astype(BF)


def solution(mesh):
    torus = Mesh(mesh.devices.reshape(NZ, NY, mesh.shape["cb"], mesh.shape["dp"]), (Z, Y, X, C))
    in_specs = (
        P((X, C), RA),
        P(X, RA),
        P(RA, X),
        P(X, RA),
        P(RA, X),
        P(RA),
        P(RA),
        P(RA),
        P(RA),
    )
    out_specs = P((X, C), RA)

    return jax.shard_map(body, mesh=torus, in_specs=in_specs, out_specs=out_specs, check_vma=False)
```
